512 devices in a mesh: sp: 32 (over z, x), tp: 16 (over y, core).
Axes of the slice: x: 4, y: 8, z: 8, core: 2. Of those that a mesh axis runs over, the one named last changes fastest.
Arguments:
- residual: bfloat16 [8192, 2048], P('sp', 'tp'), may hold values from -6 to 6
- queries: bfloat16 [8192, 1024], P('sp', 'tp'), may hold values from -5.5 to 5.5
- keys: bfloat16 [8192, 128], P('sp'), may hold values from -5.5 to 5.5
- values: bfloat16 [8192, 128], P('sp'), may hold values from -6 to 6
- documents: int32 [8192], P('sp'), may hold values from 0 to 15, never falling along the last dimension, each value on 1 to 1024 neighbouring positions
- sinks: float32 [16], P('tp'), may hold values from 1 to 6
- head_gain: float32 [1024], replicated, may hold values from 0.1 to 1.9
- out_weight: bfloat16 [1024, 2048], P(None, 'tp'), may hold values from -0.1875 to 0.1875
- norm_gain: float32 [2048], P('tp'), may hold values from 0.1 to 1.9
- norm_shift: float32 [2048], P('tp'), may hold values from -3 to 3
- routes: int32 [8192, 2], P('sp'), may hold values from 0 to 31, all different within a row; in each aligned block of 256 rows (0 to 255, 256 to 511, ...) at most 24 rows name the same one
- route_logits: float32 [8192, 2], P('sp'), may hold values from -150 to 150
- gate_weight: bfloat16 [32, 2048, 6144], P('sp', None, 'tp'), may hold values from -0.125 to 0.125
- up_weight: bfloat16 [32, 2048, 6144], P('sp', None, 'tp'), may hold values from -0.125 to 0.125
- down_weight: bfloat16 [32, 6144, 2048], P('sp', 'tp'), may hold values from -0.15625 to 0.15625
- final_gain: float32 [2048], P('tp'), may hold values from 0.1 to 1.9
- final_shift: float32 [2048], P('tp'), may hold values from -3 to 3
Outputs:
- layer_out: bfloat16 [8192, 2048], P('sp', 'tp')
The draws below stay inside these ranges and needn't reach their ends.
Inputs may be any that keep to these rules, and one draw needn't show every extreme that they name: `documents`: document numbers never fall along the sequence; each document has at least one position and at most 1024, and some document has exactly 1024. `routes`: each row names 2 different experts. In each aligned block of 256 rows (the rows of one index of sp) no expert is named by more than 24 rows, a bound that some block reaches.
All inputs are finite; a program needn't handle non-finite values.
Results may differ from the reference program's by a relative error of at most 0.014.
Values may be sent and summed in bfloat16 or wider, within the bound.
No kernel may reach another device: no remote copies, remote signals or barrier semaphores. Data moves between devices by JAX's collectives and lax.ppermute only.
A program may use at most 128 MiB of HBM per device.

```python
import math
import jax
import jax.numpy as jnp
import numpy as np
from jax import lax

D = 2048
QUERY_HEADS = 16
KEY_VALUE_HEADS = 2
HEAD_SIZE = 64
FF = 6144
WINDOW_SIZE = 128
TOP = 2
TOK_SP = 256
PACKED_TOKENS = 8192
EXPERTS = 32
CAP = 24
DOCS = 16
DOC_MOST = 1024
N_SP = 32
N_TP = 16


def drawn_sample(key, salt, head_list):
    base = jax.random.truncated_normal(jax.random.fold_in(key, salt), -5.0, 5.0, (PACKED_TOKENS, head_list, HEAD_SIZE), jnp.float32)
    return base.reshape(PACKED_TOKENS, head_list * HEAD_SIZE).astype(jnp.bfloat16)


def draw_queries(key, part):
    return drawn_sample(key, 11, QUERY_HEADS)


def draw_keys(key, part):
    return drawn_sample(key, 13, KEY_VALUE_HEADS)


def draw_route_logits(key, part):
    logits = 1.5 * jax.random.truncated_normal(jax.random.fold_in(key, 17), -4.0, 4.0, (PACKED_TOKENS, TOP), jnp.float32)
    return logits


def block_scale(stream_key, extent, pieces, smallest, largest):
    level = 1.0
    for position, blocks in pieces:
        draws = jax.random.uniform(jax.random.fold_in(jax.random.fold_in(stream_key, 6), position), (blocks,), jnp.float32, smallest / len(pieces), largest / len(pieces))
        level = level * jnp.repeat(jnp.exp(draws), extent[position] // blocks).reshape((-1,) + (1,) * (len(extent) - 1 - position))
    return level


def profile(number_of, total, bound, lean):
    weights = [(1 << 20) // math.isqrt(standing ** lean) + 1 for standing in range(2, number_of + 1)]
    spare, counts = total - bound - (number_of - 1), [1] * (number_of - 1)
    while spare > 0:
        movable = [i for i in range(number_of - 1) if counts[i] < bound]
        mass, left = sum([weights[i] for i in movable]), spare
        for i in movable:
            addition = min(bound - counts[i], max(1, left * weights[i] // mass), spare)
            counts[i] = counts[i] + addition
            spare = spare - addition
    return np.array([bound] + counts)


def uneven_parts(stream_key, number_of, total, bound, skew):
    if number_of == 2:
        one = jax.random.randint(stream_key, (), max(1, total - bound), min(bound, total - 1) + 1)
        return jnp.stack([one, total - one])
    tallies = jnp.asarray(profile(number_of, total, bound, skew), jnp.int32)
    pairs = (number_of - 1) // 2
    giver, receiver = tallies[1:1 + 2 * pairs:2], tallies[2:2 + 2 * pairs:2]
    margin = jnp.minimum(giver - 1, bound - receiver)
    moved = jax.random.randint(jax.random.fold_in(stream_key, 1), (pairs,), 0, 1 << 20) % (margin + 1)
    tallies = tallies.at[1:1 + 2 * pairs:2].set(giver - moved).at[2:2 + 2 * pairs:2].set(receiver + moved)
    return tallies[jax.random.permutation(jax.random.fold_in(stream_key, 2), number_of)]


def deal_out(key, own, number, rows, number_of, top, reach, lean):
    order = jax.random.permutation(key, number_of)
    crowded, usual = shares(number_of, rows * top, reach, lean, True), shares(number_of, rows * top, reach, lean, False)
    places = jnp.arange(number_of)

    def named(lengths, turn):
        used = int((lengths > 0).sum())
        fixed = max(1, used // 4)
        passed = fixed + (places - fixed + turn * (used - fixed)) % max(1, number_of - fixed)
        return jnp.zeros((number_of,), jnp.int32).at[order[jnp.where(places < fixed, places, passed)]].set(jnp.asarray(lengths, jnp.int32))

    lengths = jnp.where(number % 4 == 0, named(crowded, number // 4), named(usual, number - number // 4 - 1))
    mixed = jax.random.permutation(jax.random.fold_in(own, 3), number_of)
    donor, receiver = mixed[0:number_of // 2 * 2:2], mixed[1:number_of // 2 * 2:2]
    room = jnp.minimum(lengths[donor] - 1, reach - lengths[receiver]) // 2
    room = jnp.where((donor == order[0]) | (receiver == order[0]) | (lengths[receiver] == 0), 0, jnp.maximum(room, 0))
    passed = jax.random.randint(jax.random.fold_in(own, 4), (number_of // 2,), 0, 1 << 20) % (room + 1)
    lengths = lengths.at[donor].add(-passed).at[receiver].add(passed)
    members = jnp.searchsorted(jnp.cumsum(lengths), jnp.arange(rows * top), side="right").astype(jnp.int32)
    table = members.reshape(top, rows).T
    table = table[jax.random.permutation(jax.random.fold_in(own, 1), rows)]
    turn = jax.random.randint(jax.random.fold_in(own, 2), (rows, 1), 0, top)
    return jnp.take_along_axis(table, (jnp.arange(top)[None, :] + turn) % top, axis=1)


def shares(count, total, most, skew, full):
    weights = [(1 << 20) // math.isqrt(grade ** skew) + 1 for grade in range(1, count + 1)]
    largest = most if full else min(most, max(-(-total // count), total * weights[0] // sum(weights)))
    least = 1 if total - largest >= count - 1 else 0
    given, spare = [largest] + [least] * (count - 1), total - largest - least * (count - 1)
    while spare > 0:
        movable = [i for i in range(1, count) if given[i] < largest] or [i for i in range(1, count) if given[i] < most]
        whole, left = sum([weights[i] for i in movable]), spare
        for i in movable:
            extra = min(most - given[i], max(1, left * weights[i] // whole), spare)
            given[i] = given[i] + extra
            spare = spare - extra
    return np.array(given)


def scatter_about(stream_key, extent, width, bound, split=(), held_as=jnp.bfloat16):
    entries = width * jax.random.normal(stream_key, extent, jnp.float32)
    if split:
        entries = entries * block_scale(stream_key, extent, split, -0.22, 0.18)
    return jnp.clip(entries, -bound, bound).astype(held_as)


def setup_inputs(seed: int = 0) -> dict:
    streams_of = jax.random.split(jax.random.key(seed), 18)
    residual = scatter_about(streams_of[0], (PACKED_TOKENS, D), 1.0, 6.0, ((0, 32), (1, 16)))
    queries = draw_queries(jax.random.fold_in(streams_of[17], 71), 0)
    keys = draw_keys(jax.random.fold_in(streams_of[17], 71), 0)
    values = scatter_about(streams_of[3], (PACKED_TOKENS, KEY_VALUE_HEADS * HEAD_SIZE), 1.0, 6.0, ((0, 32),))
    documents = jnp.searchsorted(jnp.cumsum(uneven_parts(streams_of[4], DOCS, PACKED_TOKENS, DOC_MOST, 1)), jnp.arange(PACKED_TOKENS), side="right").astype(jnp.int32)
    sinks = jnp.clip(1.0 + 5.0 * jax.random.uniform(streams_of[5], (QUERY_HEADS,), jnp.float32) ** block_scale(streams_of[5], (QUERY_HEADS,), ((0, 16),), -0.2, 0.2), 1.0, 6.0)
    head_gain = jnp.clip(1.0 + 0.18 * jax.random.normal(streams_of[6], (QUERY_HEADS * HEAD_SIZE,), jnp.float32), 0.1, 1.9)
    out_weight = scatter_about(streams_of[7], (QUERY_HEADS * HEAD_SIZE, D), (QUERY_HEADS * HEAD_SIZE) ** -0.5, 0.1875, ((1, 16),))
    norm_gain = jnp.clip(1.0 + 0.18 * jax.random.normal(streams_of[8], (D,), jnp.float32), 0.1, 1.9)
    norm_shift = scatter_about(streams_of[9], (D,), 0.5, 3.0, ((0, 16),), jnp.float32)
    routes_keys = jax.random.split(jax.random.fold_in(streams_of[10], 1), PACKED_TOKENS // TOK_SP)
    routes_turns = jax.random.permutation(jax.random.fold_in(streams_of[10], 3), PACKED_TOKENS // TOK_SP)
    routes = jax.vmap(lambda own, number: deal_out(jax.random.fold_in(streams_of[10], 2), own, number, TOK_SP, EXPERTS, TOP, CAP, 1))(routes_keys, routes_turns).reshape((PACKED_TOKENS, TOP))
    route_logits = draw_route_logits(jax.random.fold_in(streams_of[17], 71), 0)
    gate_weight = scatter_about(streams_of[12], (EXPERTS, D, FF), D ** -0.5, 0.125, ((0, 32), (2, 16)))
    up_weight = scatter_about(streams_of[13], (EXPERTS, D, FF), D ** -0.5, 0.125, ((0, 32), (2, 16)))
    down_weight = scatter_about(streams_of[14], (EXPERTS, FF, D), (FF // 4) ** -0.5, 0.15625, ((0, 32), (1, 16)))
    final_gain = jnp.clip(1.0 + 0.18 * jax.random.normal(streams_of[15], (D,), jnp.float32), 0.1, 1.9)
    final_shift = scatter_about(streams_of[16], (D,), 0.5, 3.0, ((0, 16),), jnp.float32)
    return {"residual": residual, "queries": queries, "keys": keys, "values": values, "documents": documents, "sinks": sinks, "head_gain": head_gain, "out_weight": out_weight, "norm_gain": norm_gain, "norm_shift": norm_shift, "routes": routes, "route_logits": route_logits, "gate_weight": gate_weight, "up_weight": up_weight, "down_weight": down_weight, "final_gain": final_gain, "final_shift": final_shift}


DEEP_ALPHA = 8.0 ** 0.25
NORM_EPS = 1e-05

def layer_norm(total, gain, shift):
    center = lax.optimization_barrier(jnp.sum(total, axis=-1, keepdims=True)) / D
    spread = lax.optimization_barrier(jnp.sum(total * total, axis=-1, keepdims=True)) / D - center * center
    return (total - center) * lax.rsqrt(spread + NORM_EPS) * gain + shift

def window_attention(queries, keys, values, documents, sinks):
    query_group = QUERY_HEADS // KEY_VALUE_HEADS
    padded_key_rows = jnp.concatenate([jnp.zeros((WINDOW_SIZE, KEY_VALUE_HEADS * HEAD_SIZE), jnp.bfloat16), keys], axis=0)
    padded_value_rows = jnp.concatenate([jnp.zeros((WINDOW_SIZE, KEY_VALUE_HEADS * HEAD_SIZE), jnp.bfloat16), values], axis=0)
    pad_docs = jnp.concatenate([jnp.full((WINDOW_SIZE,), -1, jnp.int32), documents.astype(jnp.int32)], axis=0)
    query_blocks = queries.reshape(PACKED_TOKENS // WINDOW_SIZE, WINDOW_SIZE, QUERY_HEADS, HEAD_SIZE)

    def one_block(inputs):
        query_block, index = inputs
        window_begin = (index * WINDOW_SIZE).astype(jnp.int32)
        key_tile_block = lax.dynamic_slice_in_dim(padded_key_rows, window_begin, 2 * WINDOW_SIZE, 0).reshape(2 * WINDOW_SIZE, KEY_VALUE_HEADS, HEAD_SIZE)
        value_tile_block = lax.dynamic_slice_in_dim(padded_value_rows, window_begin, 2 * WINDOW_SIZE, 0).reshape(2 * WINDOW_SIZE, KEY_VALUE_HEADS, HEAD_SIZE)
        key_docs = lax.dynamic_slice_in_dim(pad_docs, window_begin, 2 * WINDOW_SIZE, 0)
        query_docs = lax.dynamic_slice_in_dim(documents.astype(jnp.int32), window_begin, WINDOW_SIZE, 0)
        key_wide = jnp.repeat(key_tile_block, query_group, axis=1)
        value_wide = jnp.repeat(value_tile_block, query_group, axis=1)
        scores = jnp.einsum('qhd,khd->hqk', query_block.astype(jnp.float32), key_wide.astype(jnp.float32)) * HEAD_SIZE ** (-0.5)
        query_pos = window_begin + jnp.arange(WINDOW_SIZE, dtype=jnp.int32)
        key_pos = window_begin - WINDOW_SIZE + jnp.arange(2 * WINDOW_SIZE, dtype=jnp.int32)
        distance = query_pos[:, None] - key_pos[None, :]
        allowed = (distance >= 0) & (distance < WINDOW_SIZE) & (key_pos[None, :] >= 0) & (query_docs[:, None] == key_docs[None, :])
        scores = jnp.where(allowed[None], scores, -jnp.inf)
        sink_col = sinks.astype(jnp.float32)[:, None]
        top = jnp.maximum(lax.optimization_barrier(jnp.max(scores, axis=-1)), sink_col)
        expd = jnp.exp(scores - top[..., None])
        probs = (expd / (lax.optimization_barrier(jnp.sum(expd, axis=-1)) + jnp.exp(sink_col - top))[..., None]).astype(jnp.bfloat16)
        result = jnp.einsum('hqk,khd->qhd', probs.astype(jnp.float32), value_wide.astype(jnp.float32))
        return result.astype(jnp.bfloat16)
    blocks = lax.map(one_block, (query_blocks, jnp.arange(PACKED_TOKENS // WINDOW_SIZE, dtype=jnp.int32)))
    return blocks.reshape(PACKED_TOKENS, QUERY_HEADS * HEAD_SIZE)

def reference(residual, queries, keys, values, documents, sinks, head_gain, out_weight, norm_gain, norm_shift, routes, route_logits, gate_weight, up_weight, down_weight, final_gain, final_shift):
    attended = window_attention(queries, keys, values, documents, sinks).astype(jnp.float32)
    scaled = (attended * lax.rsqrt(lax.optimization_barrier(jnp.mean(attended * attended, axis=-1, keepdims=True)) + NORM_EPS) * head_gain).astype(jnp.bfloat16)
    mix = jnp.dot(scaled, out_weight, preferred_element_type=jnp.float32)
    first = DEEP_ALPHA * residual.astype(jnp.float32) + mix
    hidden = layer_norm(first, norm_gain, norm_shift)
    hidden_rows = hidden.astype(jnp.bfloat16)
    flat = routes.astype(jnp.int32).reshape(N_SP, TOK_SP * TOP)
    onehot = (flat[..., None] == jnp.arange(EXPERTS, dtype=jnp.int32)).astype(jnp.int32)
    rank = lax.optimization_barrier(jnp.sum(jnp.cumsum(onehot, axis=1) * onehot, axis=-1)) - 1
    source = jnp.arange(N_SP, dtype=jnp.int32)[:, None]
    place = ((flat * N_SP + source) * CAP + rank).astype(jnp.int32)
    owner = source * TOK_SP + jnp.arange(TOK_SP * TOP, dtype=jnp.int32)[None, :] // TOP
    table = jnp.full((EXPERTS * N_SP * CAP,), PACKED_TOKENS, jnp.int32).at[place.reshape(-1)].set(owner.reshape(-1).astype(jnp.int32))
    padded = jnp.concatenate([hidden_rows, jnp.zeros((1, D), jnp.bfloat16)], axis=0)

    def one_expert(inputs):
        index_rows, gate_w, up_w, down_w = inputs
        picked_rows = padded[index_rows]
        gate = jnp.dot(picked_rows, gate_w, preferred_element_type=jnp.float32)
        up_val = jnp.dot(picked_rows, up_w, preferred_element_type=jnp.float32)
        middle = (jax.nn.silu(gate) * up_val).astype(jnp.bfloat16)
        blocks = jnp.einsum('rjf,jfd->rjd', middle.reshape(-1, N_TP, FF // N_TP).astype(jnp.float32), down_w.reshape(N_TP, FF // N_TP, D).astype(jnp.float32))
        blocks = blocks.astype(jnp.bfloat16).astype(jnp.float32)
        return lax.optimization_barrier(jnp.sum(blocks, axis=1)).astype(jnp.bfloat16)
    outputs = lax.map(one_expert, (table.reshape(EXPERTS, N_SP * CAP), gate_weight, up_weight, down_weight))
    expert_out = outputs.reshape(EXPERTS * N_SP * CAP, D)[place.reshape(-1)].reshape(PACKED_TOKENS, TOP, D).astype(jnp.float32)
    share = jax.nn.softmax(route_logits.astype(jnp.float32), axis=-1)
    moe = lax.optimization_barrier(jnp.sum(share[:, :, None] * expert_out, axis=1))
    second = DEEP_ALPHA * hidden + moe
    return layer_norm(second, final_gain, final_shift).astype(jnp.bfloat16)
```

```python
import functools

import jax
import jax.numpy as jnp
from jax import lax
from jax.experimental import pallas as pl
from jax.experimental.pallas import tpu as pltpu
from jax.sharding import Mesh, PartitionSpec as P

D = 2048
QUERY_HEADS = 16
KEY_VALUE_HEADS = 2
HEAD_SIZE = 64
WINDOW = 128
TOP = 2
TOKENS = 256
CAP = 24
N_SP = 32
N_TP = 16
SLOTS = N_SP * CAP
FF_LOCAL = 384
LANES = 128
STAT_ROWS = 8
ROWS = SLOTS + STAT_ROWS
ROW_TILE = 256

DEEP_ALPHA = 8.0**0.25
NORM_EPS = 1e-05

SP = ("z", "x")
TP = ("y", "c")
Y = 8

f32 = jnp.float32
bf16 = jnp.bfloat16


def eye():
    return lax.broadcasted_iota(jnp.int32, (LANES, LANES), 0) == lax.broadcasted_iota(
        jnp.int32, (LANES, LANES), 1
    )


def column(row):
    return jnp.sum(jnp.where(eye(), row, jnp.zeros_like(row)), axis=1, keepdims=True)


def row_of(col):
    return jnp.sum(jnp.where(eye(), col, jnp.zeros_like(col)), axis=0, keepdims=True)


def nt(a, b):
    return lax.dot_general(a, b, (((1,), (1,)), ((), ())), preferred_element_type=f32)


def high_low(v):
    high = v.astype(bf16).astype(f32)
    return high, v - high


def attention_kernel(
    sinks_ref, halo_ref, keys_ref, values_ref, queries_ref, docs_ref, residual_ref,
    weight_ref, gain_ref, shift_ref, out_ref,
):
    kv_head = (lax.axis_index("y") * 2 + lax.axis_index("c")) // (QUERY_HEADS // KEY_VALUE_HEADS)
    first_block = (lax.axis_index("z") * 4 + lax.axis_index("x")) == 0
    sink = sinks_ref[0]
    pick = kv_head == 0

    def head_of(block):
        return jnp.where(pick, block[:, :HEAD_SIZE], block[:, HEAD_SIZE:])

    keys = [head_of(halo_ref[:WINDOW, :LANES].astype(f32)).astype(bf16)]
    vals = [head_of(halo_ref[:WINDOW, LANES:].astype(f32)).astype(bf16)]
    for i in range(2):
        part = slice(i * WINDOW, (i + 1) * WINDOW)
        keys.append(head_of(keys_ref[part, :].astype(f32)).astype(bf16))
        vals.append(head_of(values_ref[part, :].astype(f32)).astype(bf16))
    docs = docs_ref[...].astype(f32)
    halo_docs = halo_ref[WINDOW : WINDOW + 8, :LANES].astype(f32)[0:1]
    halo_docs = jnp.where(first_block, -1.0, halo_docs)
    doc_rows = [halo_docs, docs[:, :WINDOW], docs[:, WINDOW:]]
    qi = lax.broadcasted_iota(jnp.int32, (WINDOW, WINDOW), 0)
    ki = lax.broadcasted_iota(jnp.int32, (WINDOW, WINDOW), 1)
    blocks = []
    for i in range(2):
        q = queries_ref[i * WINDOW : (i + 1) * WINDOW, :]
        q_docs = column(doc_rows[i + 1])
        before = nt(q, keys[i]) * HEAD_SIZE ** (-0.5)
        here = nt(q, keys[i + 1]) * HEAD_SIZE ** (-0.5)
        before = jnp.where((ki > qi) & (q_docs == doc_rows[i]), before, -jnp.inf)
        here = jnp.where((ki <= qi) & (q_docs == doc_rows[i + 1]), here, -jnp.inf)
        top = jnp.maximum(
            jnp.maximum(
                jnp.max(before, axis=1, keepdims=True), jnp.max(here, axis=1, keepdims=True)
            ),
            sink,
        )
        before, here = jnp.exp(before - top), jnp.exp(here - top)
        total = (
            jnp.sum(before, axis=1, keepdims=True)
            + jnp.sum(here, axis=1, keepdims=True)
            + jnp.exp(sink - top)
        )
        before = (before / total).astype(bf16)
        here = (here / total).astype(bf16)
        blocks.append(
            jnp.dot(before, vals[i], preferred_element_type=f32)
            + jnp.dot(here, vals[i + 1], preferred_element_type=f32)
        )
    attended = jnp.concatenate(blocks, axis=1).astype(bf16)
    ones = jnp.ones((8, LANES), bf16)
    means = nt(ones, residual_ref[...])[0:1]
    w_sums = nt(ones, weight_ref[...])[0:1]
    rows = [means[:, :LANES], means[:, LANES:]]
    rows += [w_sums[:, i * LANES : (i + 1) * LANES] for i in range(8)]
    rows += [*high_low(gain_ref[...]), *high_low(shift_ref[...])]
    rows += [jnp.zeros((2, LANES), f32)]
    tail = jnp.concatenate(rows, axis=0).astype(bf16)
    for t in range(N_TP):
        out_ref[t, :WINDOW, :] = attended
        out_ref[t, WINDOW:, :] = tail


def mix_kernel(
    gathered_ref, head_gain_ref, weight_ref, residual_ref, routes_ref,
    first_ref, outgoing_ref, stats_ref, slots_ref, affine_ref,
):
    tails = [gathered_ref[t, WINDOW:, :].astype(f32) for t in range(N_TP)]
    total = functools.reduce(jnp.add, tails)
    for t in range(N_TP):
        lanes = slice(t * LANES, (t + 1) * LANES)
        affine_ref[0:1, lanes] = tails[t][10:11] + tails[t][11:12]
        affine_ref[1:2, lanes] = tails[t][12:13] + tails[t][13:14]
    w_mean = jnp.concatenate([total[2 + i : 3 + i] for i in range(8)], axis=1)
    head_gain = head_gain_ref[...]
    firsts = []
    for h in range(2):
        lanes = slice(h * HEAD_SIZE, (h + 1) * HEAD_SIZE)
        heads = jnp.concatenate(
            [gathered_ref[t, :WINDOW, lanes].astype(f32) for t in range(N_TP)], axis=1
        )
        spread = jnp.mean(heads * heads, axis=1, keepdims=True)
        scaled = (heads * lax.rsqrt(spread + NORM_EPS) * head_gain).astype(bf16)
        mix = jnp.dot(scaled, weight_ref[...], preferred_element_type=f32)
        center = DEEP_ALPHA * column(total[h : h + 1]) + jnp.sum(
            scaled.astype(f32) * w_mean, axis=1, keepdims=True
        )
        rows = slice(h * LANES, (h + 1) * LANES)
        first = DEEP_ALPHA * residual_ref[rows, :].astype(f32) + mix - center * (1.0 / D)
        first_ref[rows, :] = first
        firsts.append(first)
    sums = [row_of(jnp.sum(f, axis=1, keepdims=True)) for f in firsts]
    squares = [row_of(jnp.sum(f * f, axis=1, keepdims=True)) for f in firsts]
    parts = [high_low(v) for v in sums + squares]
    stats_ref[...] = jnp.concatenate(
        [p[0] for p in parts] + [p[1] for p in parts], axis=0
    ).astype(bf16)
    routes = routes_ref[...]
    expert = lax.broadcasted_iota(jnp.int32, (N_SP, TOKENS), 0)
    picks = [expert == routes[r : r + 1, :] for r in range(TOP)]
    named = (picks[0] | picks[1]).astype(f32).astype(bf16)
    earlier = (
        lax.broadcasted_iota(jnp.int32, (TOKENS, TOKENS), 0)
        < lax.broadcasted_iota(jnp.int32, (TOKENS, TOKENS), 1)
    ).astype(f32).astype(bf16)
    rank = jnp.dot(named, earlier, preferred_element_type=f32)
    slots = [
        routes[r : r + 1, :] * CAP
        + jnp.sum(jnp.where(picks[r], rank, 0.0), axis=0, keepdims=True).astype(jnp.int32)
        for r in range(TOP)
    ]
    slots_ref[...] = jnp.concatenate(slots + [jnp.zeros((6, TOKENS), jnp.int32)], axis=0)
    slot = lax.broadcasted_iota(jnp.int32, (SLOTS, TOKENS), 0)
    place = ((slot == slots[0]) | (slot == slots[1])).astype(f32).astype(bf16)
    source = jnp.concatenate(firsts, axis=0).astype(bf16)
    outgoing_ref[...] = jnp.dot(place, source, preferred_element_type=f32).astype(bf16)


def expert_kernel(
    own_ref, mine_ref, other_ref, affine_ref, gate_ref, up_ref, down_ref,
    keep_ref, send_ref, rows_ref, out_ref,
):
    y, c = lax.axis_index("y"), lax.axis_index("c")
    way = 1 - 2 * c

    def lanes_of(chip, half):
        return pl.ds(pl.multiple_of((lax.rem(chip + 2 * Y, Y) * 2 + half) * LANES, LANES), LANES)

    blocks = [(own_ref, h, lanes_of(y, h)) for h in range(2)]
    for k in range(1, 4):
        for h in range(2):
            blocks.append((mine_ref, 2 * k - 2 + h, lanes_of(y - way * k, h)))
            blocks.append((other_ref, 2 * k - 2 + h, lanes_of(y + way * k, h)))
    blocks.append((mine_ref, 6, lanes_of(y + 4, c)))
    blocks.append((other_ref, 6, lanes_of(y + 4, 1 - c)))
    total = square = 0.0
    for ref, i, _ in blocks:
        v = ref[i].astype(f32)
        total = total + v
        square = square + v * v
    center = jnp.sum(total, axis=1, keepdims=True) * (1.0 / D)
    spread = jnp.sum(square, axis=1, keepdims=True) * (1.0 / D) - center * center
    scale = lax.rsqrt(spread + NORM_EPS)
    offset = center * scale
    for ref, i, lanes in blocks:
        v = ref[i].astype(f32) * scale - offset
        rows_ref[:, lanes] = (v * affine_ref[0:1, lanes] + affine_ref[1:2, lanes]).astype(bf16)
    gate = jnp.dot(rows_ref[...], gate_ref[...], preferred_element_type=f32)
    up = jnp.dot(rows_ref[...], up_ref[...], preferred_element_type=f32)
    middle = (gate / (1.0 + jnp.exp(-gate)) * up).astype(bf16)
    out_ref[...] = jnp.dot(middle, down_ref[...], preferred_element_type=f32)
    for k in range(1, 4):
        for h in range(2):
            keep_ref[2 * k - 2 + h] = out_ref[:, lanes_of(y + way * k, h)].astype(bf16)
            send_ref[2 * k - 2 + h] = out_ref[:, lanes_of(y - way * k, h)].astype(bf16)
    keep_ref[6] = out_ref[:, lanes_of(y + 4, c)].astype(bf16)
    send_ref[6] = out_ref[:, lanes_of(y + 4, 1 - c)].astype(bf16)
    keep_ref[7] = out_ref[:, lanes_of(y, c)].astype(bf16)
    send_ref[7] = out_ref[:, lanes_of(y, 1 - c)].astype(bf16)


def combine_kernel(
    returned_ref, first_ref, totals_ref, slots_ref, logits_ref, gain_ref, shift_ref,
    second_ref, stats_ref,
):
    totals = totals_ref[...]
    totals = totals[0:4] + totals[4:8]
    sums, squares = [], []
    for h in range(2):
        rows = slice(h * LANES, (h + 1) * LANES)
        center = column(totals[h : h + 1]) * (1.0 / D)
        spread = column(totals[2 + h : 3 + h]) * (1.0 / D) - center * center
        hidden = (first_ref[rows, :] - center) * lax.rsqrt(spread + NORM_EPS)
        hidden = hidden * gain_ref[...] + shift_ref[...]
        slot = lax.broadcasted_iota(jnp.int32, (LANES, SLOTS), 1).astype(f32)
        logits = [column(logits_ref[r : r + 1, rows]) for r in range(TOP)]
        top = jnp.maximum(logits[0], logits[1])
        weights = [jnp.exp(v - top) for v in logits]
        norm = weights[0] + weights[1]
        moe = 0.0
        for r in range(TOP):
            at = column(slots_ref[r : r + 1, rows].astype(f32))
            place = (slot == at).astype(f32).astype(bf16)
            picked = jnp.dot(place, returned_ref[...], preferred_element_type=f32)
            moe = moe + weights[r] / norm * picked
        second = DEEP_ALPHA * hidden + moe
        second_ref[rows, :] = second
        sums.append(row_of(jnp.sum(second, axis=1, keepdims=True)))
        squares.append(row_of(jnp.sum(second * second, axis=1, keepdims=True)))
    stats = jnp.concatenate(sums + squares + [jnp.zeros((4, LANES), f32)], axis=0)
    for t in range(N_TP):
        stats_ref[t] = stats


def norm_kernel(stats_ref, second_ref, gain_ref, shift_ref, out_ref):
    totals = functools.reduce(jnp.add, [stats_ref[t] for t in range(N_TP)])
    for h in range(2):
        rows = slice(h * LANES, (h + 1) * LANES)
        center = column(totals[h : h + 1]) * (1.0 / D)
        spread = column(totals[2 + h : 3 + h]) * (1.0 / D) - center * center
        out = (second_ref[rows, :] - center) * lax.rsqrt(spread + NORM_EPS)
        out_ref[rows, :] = (out * gain_ref[...] + shift_ref[...]).astype(bf16)


def call(kernel, outs, flops, moved, **more):
    return pl.pallas_call(
        kernel,
        out_shape=outs,
        cost_estimate=pl.CostEstimate(flops=flops, bytes_accessed=moved, transcendentals=0),
        compiler_params=pltpu.CompilerParams(vmem_limit_bytes=48 * 1024 * 1024),
        **more,
    )


def shape(dims, dtype):
    return jax.ShapeDtypeStruct(dims, dtype)


def swap(v):
    return lax.ppermute(v, "c", [(0, 1), (1, 0)])


def onward(v, distance):
    pairs = []
    for y in range(Y):
        pairs.append((2 * y, 2 * ((y + distance) % Y)))
        pairs.append((2 * y + 1, 2 * ((y - distance) % Y) + 1))
    return lax.ppermute(v, TP, pairs)


def by_core(even, odd):
    return jnp.where(lax.axis_index("c") == 0, even, odd)


def to_all(value):
    return lax.all_to_all(value, TP, 0, 0, tiled=True)


def over_sp(value):
    return lax.all_to_all(value, SP, 0, 0, tiled=True)


def gather_columns(block):
    partner = swap(block)
    own = by_core(jnp.stack([block, partner]), jnp.stack([partner, block]))
    two = onward(own, 2)
    one = onward(own, 1)
    three = onward(two, 1)
    four = onward(by_core(two[0:1], two[1:2]), 2)
    mine = jnp.concatenate([one, two, three, four], axis=0)
    return own, mine, swap(mine)


def scatter_sum(keep, send):
    total = keep.astype(f32) + swap(send).astype(f32)
    rounded = total.astype(bf16)
    three = onward(rounded[4:6], 1)
    four = onward(rounded[6:7], 2)
    one = onward(rounded[0:2], 1)
    four = four.astype(f32)
    none = jnp.zeros_like(four)
    four = by_core(jnp.concatenate([four, none]), jnp.concatenate([none, four]))
    two = onward((total[2:4] + three.astype(f32) + four).astype(bf16), 2)
    side = one.astype(f32) + two.astype(f32)
    other = swap(by_core(side[1], side[0]).astype(bf16))
    return (by_core(side[0], side[1]) + other.astype(f32) + total[7]).astype(bf16)


def local(
    residual, queries, keys, values, documents, sinks, head_gain, out_weight, norm_gain,
    norm_shift, routes, route_logits, gate_weight, up_weight, down_weight, final_gain,
    final_shift,
):
    edge = jnp.concatenate([keys[TOKENS - WINDOW :], values[TOKENS - WINDOW :]], axis=1)
    edge_docs = documents[TOKENS - WINDOW :].astype(bf16)
    edge_docs = jnp.pad(edge_docs[None], ((0, 7), (0, LANES)))
    halo = lax.ppermute(
        jnp.concatenate([edge, edge_docs], axis=0), SP, [(i - 1, i) for i in range(1, N_SP)]
    )
    gain, shift = norm_gain[None], norm_shift[None]
    whole = pl.BlockSpec(memory_space=pltpu.VMEM)
    payload = call(
        attention_kernel,
        shape((N_TP, WINDOW + 16, LANES), bf16),
        60_000_000,
        1_500_000,
        in_specs=[pl.BlockSpec(memory_space=pltpu.SMEM)] + [whole] * 9,
    )(sinks, halo, keys, values, queries, documents[None], residual, out_weight, gain, shift)
    gathered = to_all(payload)
    first, outgoing, stats, slots, affine = call(
        mix_kernel,
        (
            shape((TOKENS, LANES), f32),
            shape((SLOTS, LANES), bf16),
            shape((STAT_ROWS, LANES), bf16),
            shape((8, TOKENS), jnp.int32),
            shape((2, D), f32),
        ),
        140_000_000,
        1_500_000,
    )(gathered, head_gain[None], out_weight, residual, routes.T)
    arrived = over_sp(outgoing.reshape(N_SP, CAP, LANES)).reshape(SLOTS, LANES)
    own, mine, other = gather_columns(jnp.concatenate([arrived, stats], axis=0))
    totals = sum(jnp.sum(v[:, SLOTS:].astype(f32), axis=0) for v in (own, mine, other))

    def tile(count, width):
        return pl.BlockSpec((count, ROW_TILE, width), lambda i: (0, i, 0))

    def fixed(*dims):
        return pl.BlockSpec(dims, lambda i: (0,) * len(dims))

    keep, send = call(
        expert_kernel,
        (shape((8, SLOTS, LANES), bf16),) * 2,
        2 * SLOTS * D * FF_LOCAL * 3,
        12_000_000,
        grid=(SLOTS // ROW_TILE,),
        in_specs=[
            tile(2, LANES),
            tile(7, LANES),
            tile(7, LANES),
            fixed(2, D),
            fixed(D, FF_LOCAL),
            fixed(D, FF_LOCAL),
            fixed(FF_LOCAL, D),
        ],
        out_specs=(tile(8, LANES), tile(8, LANES)),
        scratch_shapes=[pltpu.VMEM((ROW_TILE, D), bf16), pltpu.VMEM((ROW_TILE, D), f32)],
    )(own, mine, other, affine, gate_weight[0], up_weight[0], down_weight[0])
    summed = scatter_sum(keep, send)
    returned = over_sp(summed.reshape(N_SP, CAP, LANES)).reshape(SLOTS, LANES)
    second, last = call(
        combine_kernel,
        (shape((TOKENS, LANES), f32), shape((N_TP, 8, LANES), f32)),
        110_000_000,
        800_000,
    )(returned, first, totals, slots, route_logits.T, gain, shift)
    return call(norm_kernel, shape((TOKENS, LANES), bf16), 1_000_000, 400_000)(
        to_all(last), second, final_gain[None], final_shift[None]
    )


def solution(mesh):
    physical = Mesh(mesh.devices.reshape(8, 4, Y, 2), SP + TP)
    return jax.shard_map(
        local,
        mesh=physical,
        in_specs=(
            P(SP, TP),
            P(SP, TP),
            P(SP, None),
            P(SP, None),
            P(SP),
            P(TP),
            P(),
            P(None, TP),
            P(TP),
            P(TP),
            P(SP, None),
            P(SP, None),
            P(SP, None, TP),
            P(SP, None, TP),
            P(SP, TP, None),
            P(TP),
            P(TP),
        ),
        out_specs=P(SP, TP),
        check_vma=False,
    )
```

```python
import functools

import jax
import jax.numpy as jnp
from jax import lax
from jax.experimental import pallas as pl
from jax.experimental.pallas import tpu as pltpu
from jax.sharding import Mesh, PartitionSpec as P

D = 2048
QUERY_HEADS = 16
KEY_VALUE_HEADS = 2
HEAD_SIZE = 64
WINDOW = 128
TOP = 2
TOKENS = 256
CAP = 24
N_SP = 32
N_TP = 16
SLOTS = N_SP * CAP
FF_LOCAL = 384
LANES = 128
STAT_ROWS = 8
HALF = SLOTS // 2
FULL = 67_043_328

DEEP_ALPHA = 8.0**0.25
NORM_EPS = 1e-05

SP = ("z", "x")
TP = ("y", "c")
Y = 8


f32 = jnp.float32
bf16 = jnp.bfloat16


def eye():
    return lax.broadcasted_iota(jnp.int32, (LANES, LANES), 0) == lax.broadcasted_iota(
        jnp.int32, (LANES, LANES), 1
    )


def column(row):
    return jnp.sum(jnp.where(eye(), row, jnp.zeros_like(row)), axis=1, keepdims=True)


def row_of(col):
    return jnp.sum(jnp.where(eye(), col, jnp.zeros_like(col)), axis=0, keepdims=True)


def nt(a, b):
    return lax.dot_general(a, b, (((1,), (1,)), ((), ())), preferred_element_type=f32)


def high_low(v):
    high = v.astype(bf16).astype(f32)
    return high, v - high


def fetch(pairs, sems):
    copies = [
        pltpu.make_async_copy(source, target, sems.at[i]) for i, (source, target) in enumerate(pairs)
    ]
    for copy in copies:
        copy.start()
    for copy in copies:
        copy.wait()


def halo_kernel(keys_hbm, values_hbm, docs_hbm, out_ref, keys_ref, values_ref, docs_ref, sems):
    last = pl.ds(TOKENS - WINDOW, WINDOW)
    fetch(
        (
            (keys_hbm.at[last], keys_ref),
            (values_hbm.at[last], values_ref),
            (docs_hbm, docs_ref),
        ),
        sems,
    )
    out_ref[:WINDOW, :LANES] = keys_ref[...]
    out_ref[:WINDOW, LANES:] = values_ref[...]
    docs = jnp.broadcast_to(docs_ref[:, WINDOW:].astype(f32), (8, LANES))
    out_ref[WINDOW:, :LANES] = docs.astype(bf16)
    out_ref[WINDOW:, LANES:] = jnp.zeros((8, LANES), bf16)


def prepare_kernel(
    residual_hbm, weight_hbm, gain_hbm, shift_hbm, keys_hbm, values_hbm, queries_hbm, docs_hbm,
    out_ref,
    residual_ref, weight_ref, gain_ref, shift_ref, keys_ref, values_ref, queries_ref, docs_ref,
    sems,
):
    fetch(
        (
            (weight_hbm, weight_ref),
            (residual_hbm, residual_ref),
            (keys_hbm, keys_ref),
            (values_hbm, values_ref),
            (queries_hbm, queries_ref),
            (docs_hbm, docs_ref),
            (gain_hbm, gain_ref),
            (shift_hbm, shift_ref),
        ),
        sems,
    )
    ones = jnp.ones((8, LANES), bf16)
    means = nt(ones, residual_ref[...])[0:1]
    w_sums = nt(ones, weight_ref[...])[0:1]
    rows = [means[:, :LANES], means[:, LANES:]]
    rows += [w_sums[:, i * LANES : (i + 1) * LANES] for i in range(8)]
    rows += [*high_low(gain_ref[...]), *high_low(shift_ref[...])]
    docs = docs_ref[...].astype(f32)
    rows += [docs[:, :WINDOW], docs[:, WINDOW:]]
    pick = kv_head() == 0
    heads = [head_of(pick, keys_ref[...]), head_of(pick, values_ref[...])]
    out_ref[:TOKENS, :] = jnp.concatenate(heads, axis=1)
    queries = queries_ref[...].astype(f32)
    out_ref[TOKENS : TOKENS + WINDOW, :] = jnp.concatenate(
        [queries[:, :WINDOW].T, queries[:, WINDOW:].T], axis=1
    ).astype(bf16)
    out_ref[TOKENS + WINDOW :, :] = jnp.concatenate(rows, axis=0).astype(bf16)


def kv_head():
    return (lax.axis_index("y") * 2 + lax.axis_index("c")) // (QUERY_HEADS // KEY_VALUE_HEADS)


def head_of(pick, block):
    block = block.astype(f32)
    return jnp.where(pick, block[:, :HEAD_SIZE], block[:, HEAD_SIZE:]).astype(bf16)


def attention_kernel(sinks_ref, halo_ref, prepared_ref, out_ref):
    first_block = (lax.axis_index("z") * 4 + lax.axis_index("x")) == 0
    sink = sinks_ref[0:1, 0:1]
    pick = kv_head() == 0
    keys = [head_of(pick, halo_ref[:WINDOW, :LANES])]
    vals = [head_of(pick, halo_ref[:WINDOW, LANES:])]
    for i in range(2):
        part = slice(i * WINDOW, (i + 1) * WINDOW)
        keys.append(prepared_ref[part, :HEAD_SIZE])
        vals.append(prepared_ref[part, HEAD_SIZE:])
    queries = prepared_ref[TOKENS : TOKENS + WINDOW, :]
    tail = prepared_ref[TOKENS + WINDOW :, :]
    halo_docs = halo_ref[WINDOW : WINDOW + 8, :LANES].astype(f32)[0:1]
    halo_docs = jnp.where(first_block, -1.0, halo_docs)
    docs = tail.astype(f32)
    doc_rows = [halo_docs, docs[14:15], docs[15:16]]
    qi = lax.broadcasted_iota(jnp.int32, (WINDOW, WINDOW), 0)
    ki = lax.broadcasted_iota(jnp.int32, (WINDOW, WINDOW), 1)
    blocks = []
    for i in range(2):
        q = queries[:, i * HEAD_SIZE : (i + 1) * HEAD_SIZE]
        q_docs = column(doc_rows[i + 1])
        before = nt(q, keys[i]) * HEAD_SIZE ** (-0.5)
        here = nt(q, keys[i + 1]) * HEAD_SIZE ** (-0.5)
        before = jnp.where((ki > qi) & (q_docs == doc_rows[i]), before, -jnp.inf)
        here = jnp.where((ki <= qi) & (q_docs == doc_rows[i + 1]), here, -jnp.inf)
        top = jnp.maximum(
            jnp.max(jnp.maximum(before, here), axis=1, keepdims=True), sink
        )
        before, here = jnp.exp(before - top), jnp.exp(here - top)
        total = jnp.sum(before + here, axis=1, keepdims=True) + jnp.exp(sink - top)
        before = (before / total).astype(bf16)
        here = (here / total).astype(bf16)
        blocks.append(
            jnp.dot(before, vals[i], preferred_element_type=f32)
            + jnp.dot(here, vals[i + 1], preferred_element_type=f32)
        )
    attended = jnp.concatenate(blocks, axis=1).astype(bf16)
    for t in range(N_TP):
        out_ref[t, :WINDOW, :] = attended
        out_ref[t, WINDOW:, :] = tail


def mix_kernel(
    gathered_ref, head_gain_ref, weight_ref, residual_ref, routes_ref,
    first_ref, outgoing_ref, stats_ref, slots_ref, affine_ref,
):
    tails = [gathered_ref[t, WINDOW:, :].astype(f32) for t in range(N_TP)]
    total = functools.reduce(jnp.add, tails)
    for t in range(N_TP):
        lanes = slice(t * LANES, (t + 1) * LANES)
        affine_ref[0:1, lanes] = tails[t][10:11] + tails[t][11:12]
        affine_ref[1:2, lanes] = tails[t][12:13] + tails[t][13:14]
    w_mean = jnp.concatenate([total[2 + i : 3 + i] for i in range(8)], axis=1)
    head_gain = head_gain_ref[...]
    firsts = []
    for h in range(2):
        lanes = slice(h * HEAD_SIZE, (h + 1) * HEAD_SIZE)
        heads = jnp.concatenate(
            [gathered_ref[t, :WINDOW, lanes].astype(f32) for t in range(N_TP)], axis=1
        )
        spread = jnp.mean(heads * heads, axis=1, keepdims=True)
        scaled = (heads * lax.rsqrt(spread + NORM_EPS) * head_gain).astype(bf16)
        mix = jnp.dot(scaled, weight_ref[...], preferred_element_type=f32)
        center = DEEP_ALPHA * column(total[h : h + 1]) + jnp.sum(
            scaled.astype(f32) * w_mean, axis=1, keepdims=True
        )
        rows = slice(h * LANES, (h + 1) * LANES)
        first = DEEP_ALPHA * residual_ref[rows, :].astype(f32) + mix - center * (1.0 / D)
        first_ref[rows, :] = first
        firsts.append(first)
    sums = [row_of(jnp.sum(f, axis=1, keepdims=True)) for f in firsts]
    squares = [row_of(jnp.sum(f * f, axis=1, keepdims=True)) for f in firsts]
    parts = [high_low(v) for v in sums + squares]
    stats_ref[...] = jnp.concatenate(
        [p[0] for p in parts] + [p[1] for p in parts], axis=0
    ).astype(bf16)
    routes = routes_ref[...]
    expert = lax.broadcasted_iota(jnp.int32, (N_SP, TOKENS), 0)
    picks = [expert == routes[r : r + 1, :] for r in range(TOP)]
    named = (picks[0] | picks[1]).astype(f32).astype(bf16)
    earlier = (
        lax.broadcasted_iota(jnp.int32, (TOKENS, TOKENS), 0)
        < lax.broadcasted_iota(jnp.int32, (TOKENS, TOKENS), 1)
    ).astype(f32).astype(bf16)
    rank = jnp.dot(named, earlier, preferred_element_type=f32)
    slots = [
        routes[r : r + 1, :] * CAP
        + jnp.sum(jnp.where(picks[r], rank, 0.0), axis=0, keepdims=True).astype(jnp.int32)
        for r in range(TOP)
    ]
    slots_ref[...] = jnp.concatenate(slots + [jnp.zeros((6, TOKENS), jnp.int32)], axis=0)
    slot = lax.broadcasted_iota(jnp.int32, (SLOTS, TOKENS), 0)
    place = ((slot == slots[0]) | (slot == slots[1])).astype(f32).astype(bf16)
    source = jnp.concatenate(firsts, axis=0).astype(bf16)
    outgoing_ref[...] = jnp.dot(place, source, preferred_element_type=f32).astype(bf16)


def expert_kernel(
    own_ref, near_up_ref, near_down_ref, two_up_ref, two_down_ref, four_ref, affine_ref,
    gate_ref, up_ref, down_ref, gate_other_ref, up_other_ref, down_other_ref,
    to_near_up_ref, to_near_down_ref, to_two_up_ref, to_two_down_ref, to_four_ref, to_own_ref,
    totals_ref, rows_ref,
):
    y = lax.axis_index("y")

    def lanes_of(away):
        at = lax.rem(y + away + Y, Y) * 2 * LANES
        return pl.multiple_of(at, 2 * LANES)

    blocks = []
    for ref, i, away in (
        (own_ref, 0, 0), (two_up_ref, 0, -2), (two_down_ref, 0, 2), (near_up_ref, 0, -1),
        (near_up_ref, 2, -3), (near_down_ref, 0, 1), (near_down_ref, 2, 3), (four_ref, 0, 4),
    ):
        for h in range(2):
            blocks.append((ref, i + h, pl.ds(pl.multiple_of(lanes_of(away) + h * LANES, LANES), LANES)))
    totals_ref[...] = functools.reduce(
        jnp.add, [ref[i, :STAT_ROWS, :].astype(f32) for ref, i, _ in blocks]
    )
    total = square = 0.0
    for ref, i, _ in blocks:
        v = ref[i, STAT_ROWS:, :].astype(f32)
        total = total + v
        square = square + v * v
    center = jnp.sum(total, axis=1, keepdims=True) * (1.0 / D)
    spread = jnp.sum(square, axis=1, keepdims=True) * (1.0 / D) - center * center
    scale = lax.rsqrt(spread + NORM_EPS)
    offset = center * scale
    for ref, i, lanes in blocks:
        v = ref[i, STAT_ROWS:, :].astype(f32) * scale - offset
        rows_ref[:, lanes] = (v * affine_ref[0:1, lanes] + affine_ref[1:2, lanes]).astype(bf16)
    middles = []
    for g, u in ((gate_ref, up_ref), (gate_other_ref, up_other_ref)):
        gate = jnp.dot(rows_ref[...], g[...], preferred_element_type=f32)
        up = jnp.dot(rows_ref[...], u[...], preferred_element_type=f32)
        middles.append((gate / (1.0 + jnp.exp(-gate)) * up).astype(bf16))
    for ref, i, away in (
        (to_near_up_ref, 0, 1), (to_near_up_ref, 2, 3), (to_near_down_ref, 0, -1),
        (to_near_down_ref, 2, -3), (to_four_ref, 0, 4), (to_two_up_ref, 0, 2),
        (to_two_down_ref, 0, -2), (to_own_ref, 0, 0),
    ):
        lanes = pl.ds(lanes_of(away), 2 * LANES)
        out = jnp.dot(middles[0], down_ref[:, lanes], preferred_element_type=f32)
        out = out + jnp.dot(middles[1], down_other_ref[:, lanes], preferred_element_type=f32)
        ref[i] = out[:, :LANES].astype(bf16)
        ref[i + 1] = out[:, LANES:].astype(bf16)


def combine_kernel(
    returned_ref, first_ref, totals_ref, slots_ref, logits_ref, gain_ref, shift_ref,
    second_ref, stats_ref,
):
    totals = totals_ref[...]
    totals = totals[0:4] + totals[4:8]
    sums, squares = [], []
    for h in range(2):
        rows = slice(h * LANES, (h + 1) * LANES)
        center = column(totals[h : h + 1]) * (1.0 / D)
        spread = column(totals[2 + h : 3 + h]) * (1.0 / D) - center * center
        hidden = (first_ref[rows, :] - center) * lax.rsqrt(spread + NORM_EPS)
        hidden = hidden * gain_ref[...] + shift_ref[...]
        slot = lax.broadcasted_iota(jnp.int32, (LANES, SLOTS), 1).astype(f32)
        logits = [column(logits_ref[r : r + 1, rows]) for r in range(TOP)]
        top = jnp.maximum(logits[0], logits[1])
        weights = [jnp.exp(v - top) for v in logits]
        norm = weights[0] + weights[1]
        moe = 0.0
        for r in range(TOP):
            at = column(slots_ref[r : r + 1, rows].astype(f32))
            place = (slot == at).astype(f32).astype(bf16)
            picked = jnp.dot(place, returned_ref[...], preferred_element_type=f32)
            moe = moe + weights[r] / norm * picked
        second = DEEP_ALPHA * hidden + moe
        second_ref[rows, :] = second
        sums.append(row_of(jnp.sum(second, axis=1, keepdims=True)))
        squares.append(row_of(jnp.sum(second * second, axis=1, keepdims=True)))
    stats = jnp.concatenate(sums + squares + [jnp.zeros((4, LANES), f32)], axis=0)
    for t in range(N_TP):
        stats_ref[t] = stats


def norm_kernel(stats_ref, second_ref, gain_ref, shift_ref, out_ref):
    totals = functools.reduce(jnp.add, [stats_ref[t] for t in range(N_TP)])
    for h in range(2):
        rows = slice(h * LANES, (h + 1) * LANES)
        center = column(totals[h : h + 1]) * (1.0 / D)
        spread = column(totals[2 + h : 3 + h]) * (1.0 / D) - center * center
        out = (second_ref[rows, :] - center) * lax.rsqrt(spread + NORM_EPS)
        out_ref[rows, :] = (out * gain_ref[...] + shift_ref[...]).astype(bf16)


def call(kernel, outs, flops, moved, limit=16 << 20, **more):
    return pl.pallas_call(
        kernel,
        out_shape=outs,
        cost_estimate=pl.CostEstimate(flops=flops, bytes_accessed=moved, transcendentals=0),
        compiler_params=pltpu.CompilerParams(vmem_limit_bytes=limit),
        **more,
    )


def shape(dims, dtype):
    return jax.ShapeDtypeStruct(dims, dtype)


def swap(v):
    return lax.ppermute(v, "c", [(0, 1), (1, 0)])


def along(v, distance):
    return lax.ppermute(v, "y", [(y, (y + distance) % Y) for y in range(Y)])


def onward(v, distance):
    pairs = []
    for y in range(Y):
        pairs.append((2 * y, 2 * ((y + distance) % Y)))
        pairs.append((2 * y + 1, 2 * ((y - distance) % Y) + 1))
    return lax.ppermute(v, TP, pairs)


def by_core(even, odd):
    return jnp.where(lax.axis_index("c") == 0, even, odd)


def to_all(value):
    return lax.all_to_all(value, TP, 0, 0, tiled=True)


def over_sp(value):
    return lax.all_to_all(value, SP, 0, 0, tiled=True)


def gather_columns(own):
    two_up = along(own, 2)
    two_down = along(own, -2)
    near_up = along(jnp.concatenate([own, two_up], axis=0), 1)
    near_down = along(jnp.concatenate([own, two_down], axis=0), -1)
    four = onward(by_core(two_up, two_down), 2)
    return own, near_up, near_down, two_up, two_down, four


def scatter_sum(near_up, near_down, two_up, two_down, four, own):
    four = onward(four, 2).astype(f32)
    near_up = along(near_up, 1).astype(f32)
    near_down = along(near_down, -1).astype(f32)
    none = jnp.zeros_like(four)
    two_up = two_up.astype(f32) + near_up[2:] + by_core(four, none)
    two_down = two_down.astype(f32) + near_down[2:] + by_core(none, four)
    two_up = along(two_up.astype(bf16), 2).astype(f32)
    two_down = along(two_down.astype(bf16), -2).astype(f32)
    return own.astype(f32) + near_up[:2] + near_down[:2] + two_up + two_down


def local(
    residual, queries, keys, values, documents, sinks, head_gain, out_weight, norm_gain,
    norm_shift, routes, route_logits, gate_weight, up_weight, down_weight, final_gain,
    final_shift,
):
    docs = documents[None]
    hbm = pl.BlockSpec(memory_space=pltpu.HBM)
    halo = call(
        halo_kernel,
        shape((WINDOW + 8, 2 * LANES), bf16),
        1_000,
        140_000,
        limit=FULL,
        in_specs=[hbm] * 3,
        scratch_shapes=[
            pltpu.VMEM((WINDOW, LANES), bf16),
            pltpu.VMEM((WINDOW, LANES), bf16),
            pltpu.VMEM((1, TOKENS), jnp.int32),
            pltpu.SemaphoreType.DMA((3,)),
        ],
    )(keys, values, docs)
    halo = lax.ppermute(halo, SP, [(i - 1, i) for i in range(1, N_SP)])
    gain, shift = norm_gain[None], norm_shift[None]
    prepared = call(
        prepare_kernel,
        shape((TOKENS + WINDOW + 16, LANES), bf16),
        3_000_000,
        600_000,
        limit=FULL,
        in_specs=[hbm] * 8,
        scratch_shapes=[
            pltpu.VMEM((TOKENS, LANES), bf16),
            pltpu.VMEM((1024, LANES), bf16),
            pltpu.VMEM((1, LANES), f32),
            pltpu.VMEM((1, LANES), f32),
            pltpu.VMEM((TOKENS, LANES), bf16),
            pltpu.VMEM((TOKENS, LANES), bf16),
            pltpu.VMEM((HEAD_SIZE, TOKENS), bf16),
            pltpu.VMEM((1, TOKENS), jnp.int32),
            pltpu.SemaphoreType.DMA((8,)),
        ],
    )(residual, out_weight, gain, shift, keys, values, queries.T, docs)
    payload = call(
        attention_kernel, shape((N_TP, WINDOW + 16, LANES), bf16), 60_000_000, 1_000_000
    )(jnp.broadcast_to(sinks[None], (1, LANES)), halo, prepared)
    gathered = to_all(payload)
    first, outgoing, stats, slots, affine = call(
        mix_kernel,
        (
            shape((TOKENS, LANES), f32),
            shape((SLOTS, LANES), bf16),
            shape((STAT_ROWS, LANES), bf16),
            shape((8, TOKENS), jnp.int32),
            shape((2, D), f32),
        ),
        140_000_000,
        1_500_000,
    )(gathered, head_gain[None], out_weight, residual, routes.T)
    arrived = over_sp(outgoing.reshape(N_SP, CAP, LANES)).reshape(SLOTS, LANES)
    low = jnp.concatenate([stats, arrived[:HALF]], axis=0)
    high = jnp.concatenate([stats, arrived[HALF:]], axis=0)
    stay, partner = by_core(low, high), swap(by_core(high, low))
    own = by_core(jnp.stack([stay, partner]), jnp.stack([partner, stay]))
    weights = (gate_weight[0], up_weight[0], down_weight[0])
    others = tuple(swap(w) for w in weights)
    pair = shape((2, HALF, LANES), bf16)
    quad = shape((4, HALF, LANES), bf16)
    *partial, totals = call(
        expert_kernel,
        (quad, quad, pair, pair, pair, pair, shape((STAT_ROWS, LANES), f32)),
        2 * SLOTS * D * FF_LOCAL * 3,
        16_000_000,
        limit=24 << 20,
        scratch_shapes=[pltpu.VMEM((HALF, D), bf16)],
    )(*gather_columns(own), affine, *weights, *others)
    summed = scatter_sum(*partial).astype(bf16)
    partner = swap(by_core(summed[1], summed[0]))
    stay = by_core(summed[0], summed[1])
    summed = by_core(jnp.concatenate([stay, partner]), jnp.concatenate([partner, stay]))
    returned = over_sp(summed.reshape(N_SP, CAP, LANES)).reshape(SLOTS, LANES)
    second, last = call(
        combine_kernel,
        (shape((TOKENS, LANES), f32), shape((N_TP, 8, LANES), f32)),
        110_000_000,
        800_000,
    )(returned, first, totals, slots, route_logits.T, gain, shift)
    return call(norm_kernel, shape((TOKENS, LANES), bf16), 1_000_000, 400_000)(
        to_all(last), second, final_gain[None], final_shift[None]
    )


def solution(mesh):
    physical = Mesh(mesh.devices.reshape(8, 4, Y, 2), SP + TP)
    return jax.shard_map(
        local,
        mesh=physical,
        in_specs=(
            P(SP, TP),
            P(SP, TP),
            P(SP, None),
            P(SP, None),
            P(SP),
            P(TP),
            P(),
            P(None, TP),
            P(TP),
            P(TP),
            P(SP, None),
            P(SP, None),
            P(SP, None, TP),
            P(SP, None, TP),
            P(SP, TP, None),
            P(TP),
            P(TP),
        ),
        out_specs=P(SP, TP),
        check_vma=False,
    )
```

```python
import functools

import jax
import jax.numpy as jnp
from jax import lax
from jax.experimental import pallas as pl
from jax.experimental.pallas import tpu as pltpu
from jax.sharding import Mesh, PartitionSpec as P

D = 2048
QUERY_HEADS = 16
KEY_VALUE_HEADS = 2
HEAD_SIZE = 64
WINDOW = 128
TOP = 2
TOKENS = 256
CAP = 24
N_SP = 32
N_TP = 16
SLOTS = N_SP * CAP
FF_LOCAL = 384
LANES = 128
STAT_ROWS = 8
HALF = SLOTS // 2
FULL = 67_043_328

DEEP_ALPHA = 8.0**0.25
NORM_EPS = 1e-05

SP = ("z", "x")
TP = ("y", "c")
Y = 8


f32 = jnp.float32
bf16 = jnp.bfloat16


def eye():
    return lax.broadcasted_iota(jnp.int32, (LANES, LANES), 0) == lax.broadcasted_iota(
        jnp.int32, (LANES, LANES), 1
    )


def column(row):
    return jnp.sum(jnp.where(eye(), row, jnp.zeros_like(row)), axis=1, keepdims=True)


def row_of(col):
    return jnp.sum(jnp.where(eye(), col, jnp.zeros_like(col)), axis=0, keepdims=True)


def nt(a, b):
    return lax.dot_general(a, b, (((1,), (1,)), ((), ())), preferred_element_type=f32)


def high_low(v):
    high = v.astype(bf16).astype(f32)
    return high, v - high


def fetch(pairs, sems):
    copies = [
        pltpu.make_async_copy(source, target, sems.at[i]) for i, (source, target) in enumerate(pairs)
    ]
    for copy in copies:
        copy.start()
    for copy in copies:
        copy.wait()


def halo_kernel(keys_hbm, values_hbm, docs_hbm, out_ref, keys_ref, values_ref, docs_ref, sems):
    last = pl.ds(TOKENS - WINDOW, WINDOW)
    fetch(
        (
            (keys_hbm.at[last], keys_ref),
            (values_hbm.at[last], values_ref),
            (docs_hbm, docs_ref),
        ),
        sems,
    )
    out_ref[:WINDOW, :LANES] = keys_ref[...]
    out_ref[:WINDOW, LANES:] = values_ref[...]
    docs = jnp.broadcast_to(docs_ref[:, WINDOW:].astype(f32), (8, LANES))
    out_ref[WINDOW:, :LANES] = docs.astype(bf16)
    out_ref[WINDOW:, LANES:] = jnp.zeros((8, LANES), bf16)


def prepare_kernel(
    residual_hbm, weight_hbm, gain_hbm, shift_hbm, keys_hbm, values_hbm, queries_hbm, docs_hbm,
    sinks_hbm, out_ref,
    residual_ref, weight_ref, gain_ref, shift_ref, keys_ref, values_ref, queries_ref, docs_ref,
    sinks_ref, sems,
):
    fetch(
        (
            (weight_hbm, weight_ref),
            (residual_hbm, residual_ref),
            (keys_hbm, keys_ref),
            (values_hbm, values_ref),
            (queries_hbm, queries_ref),
            (docs_hbm, docs_ref),
            (gain_hbm, gain_ref),
            (shift_hbm, shift_ref),
            (sinks_hbm, sinks_ref),
        ),
        sems,
    )
    ones = jnp.ones((8, LANES), bf16)
    means = nt(ones, residual_ref[...])[0:1]
    w_sums = nt(ones, weight_ref[...])[0:1]
    rows = [means[:, :LANES], means[:, LANES:]]
    rows += [w_sums[:, i * LANES : (i + 1) * LANES] for i in range(8)]
    rows += [*high_low(gain_ref[...]), *high_low(shift_ref[...])]
    docs = docs_ref[...].astype(f32)
    rows += [docs[:, :WINDOW], docs[:, WINDOW:]]
    sink = jnp.broadcast_to(sinks_ref[...], (1, LANES))
    rows += [*high_low(sink), jnp.zeros((6, LANES), f32)]
    pick = kv_head() == 0
    heads = [head_of(pick, keys_ref[...]), head_of(pick, values_ref[...])]
    out_ref[:TOKENS, :] = jnp.concatenate(heads, axis=1)
    queries = queries_ref[...].astype(f32)
    out_ref[TOKENS : TOKENS + WINDOW, :] = jnp.concatenate(
        [queries[:, :WINDOW].T, queries[:, WINDOW:].T], axis=1
    ).astype(bf16)
    out_ref[TOKENS + WINDOW :, :] = jnp.concatenate(rows, axis=0).astype(bf16)


def kv_head():
    return (lax.axis_index("y") * 2 + lax.axis_index("c")) // (QUERY_HEADS // KEY_VALUE_HEADS)


def head_of(pick, block):
    block = block.astype(f32)
    return jnp.where(pick, block[:, :HEAD_SIZE], block[:, HEAD_SIZE:]).astype(bf16)


def attention_kernel(halo_ref, prepared_ref, out_ref):
    first_block = (lax.axis_index("z") * 4 + lax.axis_index("x")) == 0
    pick = kv_head() == 0
    keys = [head_of(pick, halo_ref[:WINDOW, :LANES])]
    vals = [head_of(pick, halo_ref[:WINDOW, LANES:])]
    for i in range(2):
        part = slice(i * WINDOW, (i + 1) * WINDOW)
        keys.append(prepared_ref[part, :HEAD_SIZE])
        vals.append(prepared_ref[part, HEAD_SIZE:])
    queries = prepared_ref[TOKENS : TOKENS + WINDOW, :]
    tail = prepared_ref[TOKENS + WINDOW : TOKENS + WINDOW + 16, :]
    sink = prepared_ref[TOKENS + WINDOW + 16 :, :].astype(f32)
    sink = (sink[0:1] + sink[1:2])[:, 0:1]
    halo_docs = halo_ref[WINDOW : WINDOW + 8, :LANES].astype(f32)[0:1]
    halo_docs = jnp.where(first_block, -1.0, halo_docs)
    docs = tail.astype(f32)
    doc_rows = [halo_docs, docs[14:15], docs[15:16]]
    qi = lax.broadcasted_iota(jnp.int32, (WINDOW, WINDOW), 0)
    ki = lax.broadcasted_iota(jnp.int32, (WINDOW, WINDOW), 1)
    blocks = []
    for i in range(2):
        q = queries[:, i * HEAD_SIZE : (i + 1) * HEAD_SIZE]
        q_docs = column(doc_rows[i + 1])
        before = nt(q, keys[i]) * HEAD_SIZE ** (-0.5)
        here = nt(q, keys[i + 1]) * HEAD_SIZE ** (-0.5)
        before = jnp.where((ki > qi) & (q_docs == doc_rows[i]), before, -jnp.inf)
        here = jnp.where((ki <= qi) & (q_docs == doc_rows[i + 1]), here, -jnp.inf)
        top = jnp.maximum(
            jnp.max(jnp.maximum(before, here), axis=1, keepdims=True), sink
        )
        before, here = jnp.exp(before - top), jnp.exp(here - top)
        total = jnp.sum(before + here, axis=1, keepdims=True) + jnp.exp(sink - top)
        before = (before / total).astype(bf16)
        here = (here / total).astype(bf16)
        blocks.append(
            jnp.dot(before, vals[i], preferred_element_type=f32)
            + jnp.dot(here, vals[i + 1], preferred_element_type=f32)
        )
    attended = jnp.concatenate(blocks, axis=1).astype(bf16)
    for t in range(Y):
        out_ref[t, :WINDOW, :] = attended
        out_ref[t, WINDOW:, :] = tail


def mix_kernel(
    mine_ref, other_ref, head_gain_ref, weight_ref, residual_ref, routes_ref,
    first_ref, outgoing_ref, stats_ref, slots_ref, affine_ref,
):
    even = lax.axis_index("c") == 0

    def sent_by(t, *at):
        pair = mine_ref[t // 2, *at].astype(f32), other_ref[t // 2, *at].astype(f32)
        return jnp.where(even, *pair) if t % 2 == 0 else jnp.where(even, *pair[::-1])

    tails = [sent_by(t, slice(WINDOW, None), slice(None)) for t in range(N_TP)]
    total = functools.reduce(jnp.add, tails)
    for t in range(N_TP):
        lanes = slice(t * LANES, (t + 1) * LANES)
        affine_ref[0:1, lanes] = tails[t][10:11] + tails[t][11:12]
        affine_ref[1:2, lanes] = tails[t][12:13] + tails[t][13:14]
    w_mean = jnp.concatenate([total[2 + i : 3 + i] for i in range(8)], axis=1)
    head_gain = head_gain_ref[...]
    firsts = []
    for h in range(2):
        lanes = slice(h * HEAD_SIZE, (h + 1) * HEAD_SIZE)
        heads = jnp.concatenate(
            [sent_by(t, slice(0, WINDOW), lanes) for t in range(N_TP)], axis=1
        )
        spread = jnp.mean(heads * heads, axis=1, keepdims=True)
        scaled = (heads * lax.rsqrt(spread + NORM_EPS) * head_gain).astype(bf16)
        mix = jnp.dot(scaled, weight_ref[...], preferred_element_type=f32)
        center = DEEP_ALPHA * column(total[h : h + 1]) + jnp.sum(
            scaled.astype(f32) * w_mean, axis=1, keepdims=True
        )
        rows = slice(h * LANES, (h + 1) * LANES)
        first = DEEP_ALPHA * residual_ref[rows, :].astype(f32) + mix - center * (1.0 / D)
        first_ref[rows, :] = first
        firsts.append(first)
    sums = [row_of(jnp.sum(f, axis=1, keepdims=True)) for f in firsts]
    squares = [row_of(jnp.sum(f * f, axis=1, keepdims=True)) for f in firsts]
    parts = [high_low(v) for v in sums + squares]
    stats_ref[...] = jnp.concatenate(
        [p[0] for p in parts] + [p[1] for p in parts], axis=0
    ).astype(bf16)
    routes = routes_ref[...]
    expert = lax.broadcasted_iota(jnp.int32, (N_SP, TOKENS), 0)
    picks = [expert == routes[r : r + 1, :] for r in range(TOP)]
    named = (picks[0] | picks[1]).astype(f32).astype(bf16)
    earlier = (
        lax.broadcasted_iota(jnp.int32, (TOKENS, TOKENS), 0)
        < lax.broadcasted_iota(jnp.int32, (TOKENS, TOKENS), 1)
    ).astype(f32).astype(bf16)
    rank = jnp.dot(named, earlier, preferred_element_type=f32)
    slots = [
        routes[r : r + 1, :] * CAP
        + jnp.sum(jnp.where(picks[r], rank, 0.0), axis=0, keepdims=True).astype(jnp.int32)
        for r in range(TOP)
    ]
    slots_ref[...] = jnp.concatenate(slots + [jnp.zeros((6, TOKENS), jnp.int32)], axis=0)
    slot = lax.broadcasted_iota(jnp.int32, (SLOTS, TOKENS), 0)
    place = ((slot == slots[0]) | (slot == slots[1])).astype(f32).astype(bf16)
    source = jnp.concatenate(firsts, axis=0).astype(bf16)
    outgoing_ref[...] = jnp.dot(place, source, preferred_element_type=f32).astype(bf16)


def expert_kernel(
    own_ref, mine_ref, other_ref, affine_ref,
    gate_ref, up_ref, down_ref, gate_other_ref, up_other_ref, down_other_ref,
    to_near_up_ref, to_near_down_ref, to_two_up_ref, to_two_down_ref, to_four_ref, to_own_ref,
    totals_ref, rows_ref,
):
    y, c = lax.axis_index("y"), lax.axis_index("c")
    way = 1 - 2 * c
    held = pl.ds(pl.multiple_of(c * HALF, HALF), HALF)

    def lanes_of(away):
        at = lax.rem(y + away + Y, Y) * 2 * LANES
        return pl.multiple_of(at, 2 * LANES)

    def lanes_at(away, half):
        return pl.ds(pl.multiple_of(lanes_of(away) + half * LANES, LANES), LANES)

    blocks = [(own_ref, h, held, lanes_at(0, h)) for h in range(2)]
    for k in range(1, 4):
        for h in range(2):
            blocks.append((mine_ref, 2 * k - 2 + h, held, lanes_at(-way * k, h)))
            blocks.append((other_ref, 2 * k - 2 + h, slice(0, HALF), lanes_at(way * k, h)))
    blocks.append((mine_ref, 6, held, lanes_at(4, c)))
    blocks.append((other_ref, 6, slice(0, HALF), lanes_at(4, 1 - c)))
    totals_ref[...] = functools.reduce(
        jnp.add,
        [
            ref[i, HALF if ref is other_ref else SLOTS :, :].astype(f32)
            for ref, i, _, _ in blocks
        ],
    )
    total = square = 0.0
    for ref, i, rows, _ in blocks:
        v = ref[i, rows, :].astype(f32)
        total = total + v
        square = square + v * v
    center = jnp.sum(total, axis=1, keepdims=True) * (1.0 / D)
    spread = jnp.sum(square, axis=1, keepdims=True) * (1.0 / D) - center * center
    scale = lax.rsqrt(spread + NORM_EPS)
    offset = center * scale
    for ref, i, rows, lanes in blocks:
        v = ref[i, rows, :].astype(f32) * scale - offset
        rows_ref[:, lanes] = (v * affine_ref[0:1, lanes] + affine_ref[1:2, lanes]).astype(bf16)
    middles = []
    for g, u in ((gate_ref, up_ref), (gate_other_ref, up_other_ref)):
        gate = jnp.dot(rows_ref[...], g[...], preferred_element_type=f32)
        up = jnp.dot(rows_ref[...], u[...], preferred_element_type=f32)
        middles.append((gate / (1.0 + jnp.exp(-gate)) * up).astype(bf16))
    for ref, i, away in (
        (to_near_up_ref, 0, 1), (to_near_up_ref, 2, 3), (to_near_down_ref, 0, -1),
        (to_near_down_ref, 2, -3), (to_four_ref, 0, 4), (to_two_up_ref, 0, 2),
        (to_two_down_ref, 0, -2), (to_own_ref, 0, 0),
    ):
        lanes = pl.ds(lanes_of(away), 2 * LANES)
        out = jnp.dot(middles[0], down_ref[:, lanes], preferred_element_type=f32)
        out = out + jnp.dot(middles[1], down_other_ref[:, lanes], preferred_element_type=f32)
        ref[i] = out[:, :LANES].astype(bf16)
        ref[i + 1] = out[:, LANES:].astype(bf16)


def combine_kernel(
    returned_ref, first_ref, totals_ref, slots_ref, logits_ref, gain_ref, shift_ref,
    second_ref, stats_ref,
):
    totals = totals_ref[...]
    totals = totals[0:4] + totals[4:8]
    sums, squares = [], []
    for h in range(2):
        rows = slice(h * LANES, (h + 1) * LANES)
        center = column(totals[h : h + 1]) * (1.0 / D)
        spread = column(totals[2 + h : 3 + h]) * (1.0 / D) - center * center
        hidden = (first_ref[rows, :] - center) * lax.rsqrt(spread + NORM_EPS)
        hidden = hidden * gain_ref[...] + shift_ref[...]
        slot = lax.broadcasted_iota(jnp.int32, (LANES, SLOTS), 1).astype(f32)
        logits = [column(logits_ref[r : r + 1, rows]) for r in range(TOP)]
        top = jnp.maximum(logits[0], logits[1])
        weights = [jnp.exp(v - top) for v in logits]
        norm = weights[0] + weights[1]
        moe = 0.0
        for r in range(TOP):
            at = column(slots_ref[r : r + 1, rows].astype(f32))
            place = (slot == at).astype(f32).astype(bf16)
            picked = jnp.dot(place, returned_ref[...], preferred_element_type=f32)
            moe = moe + weights[r] / norm * picked
        second = DEEP_ALPHA * hidden + moe
        second_ref[rows, :] = second
        sums.append(row_of(jnp.sum(second, axis=1, keepdims=True)))
        squares.append(row_of(jnp.sum(second * second, axis=1, keepdims=True)))
    stats = jnp.concatenate(sums + squares + [jnp.zeros((4, LANES), f32)], axis=0)
    for t in range(N_TP):
        stats_ref[t] = stats


def norm_kernel(stats_ref, second_ref, gain_ref, shift_ref, out_ref):
    totals = functools.reduce(jnp.add, [stats_ref[t] for t in range(N_TP)])
    for h in range(2):
        rows = slice(h * LANES, (h + 1) * LANES)
        center = column(totals[h : h + 1]) * (1.0 / D)
        spread = column(totals[2 + h : 3 + h]) * (1.0 / D) - center * center
        out = (second_ref[rows, :] - center) * lax.rsqrt(spread + NORM_EPS)
        out_ref[rows, :] = (out * gain_ref[...] + shift_ref[...]).astype(bf16)


def call(kernel, outs, flops, moved, limit=16 << 20, **more):
    return pl.pallas_call(
        kernel,
        out_shape=outs,
        cost_estimate=pl.CostEstimate(flops=flops, bytes_accessed=moved, transcendentals=0),
        compiler_params=pltpu.CompilerParams(vmem_limit_bytes=limit),
        **more,
    )


def shape(dims, dtype):
    return jax.ShapeDtypeStruct(dims, dtype)


def swap(v):
    return lax.ppermute(v, "c", [(0, 1), (1, 0)])


def along(v, distance):
    return lax.ppermute(v, "y", [(y, (y + distance) % Y) for y in range(Y)])


def onward(v, distance):
    pairs = []
    for y in range(Y):
        pairs.append((2 * y, 2 * ((y + distance) % Y)))
        pairs.append((2 * y + 1, 2 * ((y - distance) % Y) + 1))
    return lax.ppermute(v, TP, pairs)


def by_core(even, odd):
    return jnp.where(lax.axis_index("c") == 0, even, odd)


def to_all(value):
    return lax.all_to_all(value, TP, 0, 0, tiled=True)


def over_sp(value):
    return lax.all_to_all(value, SP, 0, 0, tiled=True)


def gather_columns(own):
    two = onward(own, 2)
    one = onward(own, 1)
    three = onward(two, 1)
    four = onward(by_core(two[0:1], two[1:2]), 2)
    mine = jnp.concatenate([one, two, three, four], axis=0)
    passed = by_core(mine[:, HALF:SLOTS], mine[:, :HALF])
    return own, mine, swap(jnp.concatenate([passed, mine[:, SLOTS:]], axis=1))


def scatter_sum(near_up, near_down, two_up, two_down, four, own):
    four = onward(four, 2).astype(f32)
    near_up = along(near_up, 1).astype(f32)
    near_down = along(near_down, -1).astype(f32)
    none = jnp.zeros_like(four)
    two_up = two_up.astype(f32) + near_up[2:] + by_core(four, none)
    two_down = two_down.astype(f32) + near_down[2:] + by_core(none, four)
    two_up = along(two_up.astype(bf16), 2).astype(f32)
    two_down = along(two_down.astype(bf16), -2).astype(f32)
    return own.astype(f32) + near_up[:2] + near_down[:2] + two_up + two_down


def local(
    residual, queries, keys, values, documents, sinks, head_gain, out_weight, norm_gain,
    norm_shift, routes, route_logits, gate_weight, up_weight, down_weight, final_gain,
    final_shift,
):
    docs = documents[None]
    hbm = pl.BlockSpec(memory_space=pltpu.HBM)
    halo = call(
        halo_kernel,
        shape((WINDOW + 8, 2 * LANES), bf16),
        1_000,
        140_000,
        limit=FULL - 160_000,
        in_specs=[hbm] * 3,
        scratch_shapes=[
            pltpu.VMEM((WINDOW, LANES), bf16),
            pltpu.VMEM((WINDOW, LANES), bf16),
            pltpu.VMEM((1, TOKENS), jnp.int32),
            pltpu.SemaphoreType.DMA((3,)),
        ],
    )(keys, values, docs)
    halo = lax.ppermute(halo, SP, [(i - 1, i) for i in range(1, N_SP)])
    gain, shift = norm_gain[None], norm_shift[None]
    prepared = call(
        prepare_kernel,
        shape((TOKENS + WINDOW + 24, LANES), bf16),
        3_000_000,
        600_000,
        limit=FULL - 240_000,
        in_specs=[hbm] * 9,
        scratch_shapes=[
            pltpu.VMEM((TOKENS, LANES), bf16),
            pltpu.VMEM((1024, LANES), bf16),
            pltpu.VMEM((1, LANES), f32),
            pltpu.VMEM((1, LANES), f32),
            pltpu.VMEM((TOKENS, LANES), bf16),
            pltpu.VMEM((TOKENS, LANES), bf16),
            pltpu.VMEM((HEAD_SIZE, TOKENS), bf16),
            pltpu.VMEM((1, TOKENS), jnp.int32),
            pltpu.VMEM((1, 1), f32),
            pltpu.SemaphoreType.DMA((9,)),
        ],
    )(residual, out_weight, gain, shift, keys, values, queries.T, docs, sinks[None])
    payload = call(
        attention_kernel, shape((Y, WINDOW + 16, LANES), bf16), 60_000_000, 1_000_000
    )(halo, prepared)
    gathered = lax.all_to_all(payload, "y", 0, 0, tiled=True)
    first, outgoing, stats, slots, affine = call(
        mix_kernel,
        (
            shape((TOKENS, LANES), f32),
            shape((SLOTS, LANES), bf16),
            shape((STAT_ROWS, LANES), bf16),
            shape((8, TOKENS), jnp.int32),
            shape((2, D), f32),
        ),
        140_000_000,
        1_500_000,
    )(gathered, swap(gathered), head_gain[None], out_weight, residual, routes.T)
    arrived = over_sp(outgoing.reshape(N_SP, CAP, LANES)).reshape(SLOTS, LANES)
    block = jnp.concatenate([arrived, stats], axis=0)
    partner = swap(block)
    own = by_core(jnp.stack([block, partner]), jnp.stack([partner, block]))
    weights = (gate_weight[0], up_weight[0], down_weight[0])
    others = tuple(swap(w) for w in weights)
    pair = shape((2, HALF, LANES), bf16)
    quad = shape((4, HALF, LANES), bf16)
    *partial, totals = call(
        expert_kernel,
        (quad, quad, pair, pair, pair, pair, shape((STAT_ROWS, LANES), f32)),
        2 * SLOTS * D * FF_LOCAL * 3,
        16_000_000,
        limit=24 << 20,
        scratch_shapes=[pltpu.VMEM((HALF, D), bf16)],
    )(*gather_columns(own), affine, *weights, *others)
    summed = scatter_sum(*partial).astype(bf16)
    partner = swap(by_core(summed[1], summed[0]))
    stay = by_core(summed[0], summed[1])
    summed = by_core(jnp.concatenate([stay, partner]), jnp.concatenate([partner, stay]))
    returned = over_sp(summed.reshape(N_SP, CAP, LANES)).reshape(SLOTS, LANES)
    second, last = call(
        combine_kernel,
        (shape((TOKENS, LANES), f32), shape((N_TP, 8, LANES), f32)),
        110_000_000,
        800_000,
    )(returned, first, totals, slots, route_logits.T, gain, shift)
    return call(norm_kernel, shape((TOKENS, LANES), bf16), 1_000_000, 400_000)(
        to_all(last), second, final_gain[None], final_shift[None]
    )


def solution(mesh):
    physical = Mesh(mesh.devices.reshape(8, 4, Y, 2), SP + TP)
    return jax.shard_map(
        local,
        mesh=physical,
        in_specs=(
            P(SP, TP),
            P(SP, TP),
            P(SP, None),
            P(SP, None),
            P(SP),
            P(TP),
            P(),
            P(None, TP),
            P(TP),
            P(TP),
            P(SP, None),
            P(SP, None),
            P(SP, None, TP),
            P(SP, None, TP),
            P(SP, TP, None),
            P(TP),
            P(TP),
        ),
        out_specs=P(SP, TP),
        check_vma=False,
    )
```

```python
import functools

import jax
import jax.numpy as jnp
from jax import lax
from jax.experimental import pallas as pl
from jax.experimental.pallas import tpu as pltpu
from jax.sharding import Mesh, PartitionSpec as P

D = 2048
QUERY_HEADS = 16
KEY_VALUE_HEADS = 2
HEAD_SIZE = 64
WINDOW = 128
TOP = 2
TOKENS = 256
CAP = 24
N_SP = 32
N_TP = 16
SLOTS = N_SP * CAP
FF_LOCAL = 384
LANES = 128
STAT_ROWS = 8
HALF = SLOTS // 2
FULL = 67_043_328

DEEP_ALPHA = 8.0**0.25
NORM_EPS = 1e-05

SP = ("z", "x")
TP = ("y", "c")
Y = 8


f32 = jnp.float32
bf16 = jnp.bfloat16


def eye():
    return lax.broadcasted_iota(jnp.int32, (LANES, LANES), 0) == lax.broadcasted_iota(
        jnp.int32, (LANES, LANES), 1
    )


def column(row):
    return jnp.sum(jnp.where(eye(), row, jnp.zeros_like(row)), axis=1, keepdims=True)


def row_of(col):
    return jnp.sum(jnp.where(eye(), col, jnp.zeros_like(col)), axis=0, keepdims=True)


def nt(a, b):
    return lax.dot_general(a, b, (((1,), (1,)), ((), ())), preferred_element_type=f32)


def high_low(v):
    high = v.astype(bf16).astype(f32)
    return high, v - high


def fetch(pairs, sems):
    copies = [
        pltpu.make_async_copy(source, target, sems.at[i]) for i, (source, target) in enumerate(pairs)
    ]
    for copy in copies:
        copy.start()
    for copy in copies:
        copy.wait()


def halo_kernel(keys_hbm, values_hbm, docs_hbm, out_ref, keys_ref, values_ref, docs_ref, sems):
    last = pl.ds(TOKENS - WINDOW, WINDOW)
    fetch(
        (
            (keys_hbm.at[last], keys_ref),
            (values_hbm.at[last], values_ref),
            (docs_hbm, docs_ref),
        ),
        sems,
    )
    out_ref[:WINDOW, :LANES] = keys_ref[...]
    out_ref[:WINDOW, LANES:] = values_ref[...]
    docs = jnp.broadcast_to(docs_ref[:, WINDOW:].astype(f32), (8, LANES))
    out_ref[WINDOW:, :LANES] = docs.astype(bf16)
    out_ref[WINDOW:, LANES:] = jnp.zeros((8, LANES), bf16)


def prepare_kernel(
    residual_hbm, weight_hbm, gain_hbm, shift_hbm, keys_hbm, values_hbm, queries_hbm, docs_hbm,
    sinks_hbm, out_ref,
    residual_ref, weight_ref, gain_ref, shift_ref, keys_ref, values_ref, queries_ref, docs_ref,
    sinks_ref, sems,
):
    fetch(
        (
            (weight_hbm, weight_ref),
            (residual_hbm, residual_ref),
            (keys_hbm, keys_ref),
            (values_hbm, values_ref),
            (queries_hbm, queries_ref),
            (docs_hbm, docs_ref),
            (gain_hbm, gain_ref),
            (shift_hbm, shift_ref),
            (sinks_hbm, sinks_ref),
        ),
        sems,
    )
    ones = jnp.ones((8, LANES), bf16)
    means = nt(ones, residual_ref[...])[0:1]
    w_sums = nt(ones, weight_ref[...])[0:1]
    rows = [means[:, :LANES], means[:, LANES:]]
    rows += [w_sums[:, i * LANES : (i + 1) * LANES] for i in range(8)]
    rows += [*high_low(gain_ref[...]), *high_low(shift_ref[...])]
    docs = docs_ref[...].astype(f32)
    rows += [docs[:, :WINDOW], docs[:, WINDOW:]]
    sink = jnp.broadcast_to(sinks_ref[...], (1, LANES))
    rows += [*high_low(sink), jnp.zeros((6, LANES), f32)]
    pick = kv_head() == 0
    heads = [head_of(pick, keys_ref[...]), head_of(pick, values_ref[...])]
    out_ref[:TOKENS, :] = jnp.concatenate(heads, axis=1)
    queries = queries_ref[...].astype(f32)
    out_ref[TOKENS : TOKENS + WINDOW, :] = jnp.concatenate(
        [queries[:, :WINDOW].T, queries[:, WINDOW:].T], axis=1
    ).astype(bf16)
    out_ref[TOKENS + WINDOW :, :] = jnp.concatenate(rows, axis=0).astype(bf16)


def kv_head():
    return (lax.axis_index("y") * 2 + lax.axis_index("c")) // (QUERY_HEADS // KEY_VALUE_HEADS)


def head_of(pick, block):
    block = block.astype(f32)
    return jnp.where(pick, block[:, :HEAD_SIZE], block[:, HEAD_SIZE:]).astype(bf16)


def attention_kernel(halo_ref, prepared_ref, out_ref):
    first_block = (lax.axis_index("z") * 4 + lax.axis_index("x")) == 0
    pick = kv_head() == 0
    keys = [head_of(pick, halo_ref[:WINDOW, :LANES])]
    vals = [head_of(pick, halo_ref[:WINDOW, LANES:])]
    for i in range(2):
        part = slice(i * WINDOW, (i + 1) * WINDOW)
        keys.append(prepared_ref[part, :HEAD_SIZE])
        vals.append(prepared_ref[part, HEAD_SIZE:])
    queries = prepared_ref[TOKENS : TOKENS + WINDOW, :]
    tail = prepared_ref[TOKENS + WINDOW : TOKENS + WINDOW + 16, :]
    sink = prepared_ref[TOKENS + WINDOW + 16 :, :].astype(f32)
    sink = (sink[0:1] + sink[1:2])[:, 0:1]
    halo_docs = halo_ref[WINDOW : WINDOW + 8, :LANES].astype(f32)[0:1]
    halo_docs = jnp.where(first_block, -1.0, halo_docs)
    docs = tail.astype(f32)
    doc_rows = [halo_docs, docs[14:15], docs[15:16]]
    qi = lax.broadcasted_iota(jnp.int32, (WINDOW, WINDOW), 0)
    ki = lax.broadcasted_iota(jnp.int32, (WINDOW, WINDOW), 1)
    blocks = []
    for i in range(2):
        q = queries[:, i * HEAD_SIZE : (i + 1) * HEAD_SIZE]
        q_docs = column(doc_rows[i + 1])
        before = nt(q, keys[i]) * HEAD_SIZE ** (-0.5)
        here = nt(q, keys[i + 1]) * HEAD_SIZE ** (-0.5)
        before = jnp.where((ki > qi) & (q_docs == doc_rows[i]), before, -jnp.inf)
        here = jnp.where((ki <= qi) & (q_docs == doc_rows[i + 1]), here, -jnp.inf)
        top = jnp.maximum(
            jnp.max(jnp.maximum(before, here), axis=1, keepdims=True), sink
        )
        before, here = jnp.exp(before - top), jnp.exp(here - top)
        total = jnp.sum(before + here, axis=1, keepdims=True) + jnp.exp(sink - top)
        before = (before / total).astype(bf16)
        here = (here / total).astype(bf16)
        blocks.append(
            jnp.dot(before, vals[i], preferred_element_type=f32)
            + jnp.dot(here, vals[i + 1], preferred_element_type=f32)
        )
    attended = jnp.concatenate(blocks, axis=1).astype(bf16)
    for t in range(Y):
        out_ref[t, :WINDOW, :] = attended
        out_ref[t, WINDOW:, :] = tail


def mix_kernel(
    mine_ref, other_ref, head_gain_ref, weight_ref, residual_ref, routes_ref,
    first_ref, outgoing_ref, stats_ref, slots_ref, affine_ref,
):
    even = lax.axis_index("c") == 0

    def sent_by(t, *at):
        pair = mine_ref[t // 2, *at].astype(f32), other_ref[t // 2, *at].astype(f32)
        return jnp.where(even, *pair) if t % 2 == 0 else jnp.where(even, *pair[::-1])

    tails = [sent_by(t, slice(WINDOW, None), slice(None)) for t in range(N_TP)]
    total = functools.reduce(jnp.add, tails)
    for t in range(N_TP):
        lanes = slice(t * LANES, (t + 1) * LANES)
        affine_ref[0:1, lanes] = tails[t][10:11] + tails[t][11:12]
        affine_ref[1:2, lanes] = tails[t][12:13] + tails[t][13:14]
    w_mean = jnp.concatenate([total[2 + i : 3 + i] for i in range(8)], axis=1)
    head_gain = head_gain_ref[...]
    firsts = []
    for h in range(2):
        lanes = slice(h * HEAD_SIZE, (h + 1) * HEAD_SIZE)
        heads = jnp.concatenate(
            [sent_by(t, slice(0, WINDOW), lanes) for t in range(N_TP)], axis=1
        )
        spread = jnp.mean(heads * heads, axis=1, keepdims=True)
        scaled = (heads * lax.rsqrt(spread + NORM_EPS) * head_gain).astype(bf16)
        mix = jnp.dot(scaled, weight_ref[...], preferred_element_type=f32)
        center = DEEP_ALPHA * column(total[h : h + 1]) + jnp.sum(
            scaled.astype(f32) * w_mean, axis=1, keepdims=True
        )
        rows = slice(h * LANES, (h + 1) * LANES)
        first = DEEP_ALPHA * residual_ref[rows, :].astype(f32) + mix - center * (1.0 / D)
        first_ref[rows, :] = first
        firsts.append(first)
    sums = [row_of(jnp.sum(f, axis=1, keepdims=True)) for f in firsts]
    squares = [row_of(jnp.sum(f * f, axis=1, keepdims=True)) for f in firsts]
    parts = [high_low(v) for v in sums + squares]
    stats_ref[...] = jnp.concatenate(
        [p[0] for p in parts] + [p[1] for p in parts], axis=0
    ).astype(bf16)
    routes = routes_ref[...]
    expert = lax.broadcasted_iota(jnp.int32, (N_SP, TOKENS), 0)
    picks = [expert == routes[r : r + 1, :] for r in range(TOP)]
    named = (picks[0] | picks[1]).astype(f32).astype(bf16)
    earlier = (
        lax.broadcasted_iota(jnp.int32, (TOKENS, TOKENS), 0)
        < lax.broadcasted_iota(jnp.int32, (TOKENS, TOKENS), 1)
    ).astype(f32).astype(bf16)
    rank = jnp.dot(named, earlier, preferred_element_type=f32)
    slots = [
        routes[r : r + 1, :] * CAP
        + jnp.sum(jnp.where(picks[r], rank, 0.0), axis=0, keepdims=True).astype(jnp.int32)
        for r in range(TOP)
    ]
    slots_ref[...] = jnp.concatenate(slots + [jnp.zeros((6, TOKENS), jnp.int32)], axis=0)
    slot = lax.broadcasted_iota(jnp.int32, (SLOTS, TOKENS), 0)
    place = ((slot == slots[0]) | (slot == slots[1])).astype(f32).astype(bf16)
    source = jnp.concatenate(firsts, axis=0).astype(bf16)
    outgoing_ref[...] = jnp.dot(place, source, preferred_element_type=f32).astype(bf16)


def block_kernel(arrived_ref, stats_ref, out_ref):
    out_ref[:SLOTS, :] = arrived_ref[...]
    out_ref[SLOTS:, :] = stats_ref[...]


def own_kernel(block_ref, partner_ref, out_ref):
    even = lax.axis_index("c") == 0

    @pl.when(even)
    def _():
        out_ref[0] = block_ref[...]
        out_ref[1] = partner_ref[...]

    @pl.when(jnp.logical_not(even))
    def _():
        out_ref[0] = partner_ref[...]
        out_ref[1] = block_ref[...]


def expert_kernel(
    own_ref, mine_ref, other_ref, affine_ref,
    gate_ref, up_ref, down_ref, gate_other_ref, up_other_ref, down_other_ref,
    middle_ref, send_ref, totals_ref, rows_ref,
):
    y, c = lax.axis_index("y"), lax.axis_index("c")
    way = 1 - 2 * c
    held = pl.ds(pl.multiple_of(c * HALF, HALF), HALF)

    def lanes_of(away):
        at = lax.rem(y + away + Y, Y) * 2 * LANES
        return pl.multiple_of(at, 2 * LANES)

    def lanes_at(away, half):
        return pl.ds(pl.multiple_of(lanes_of(away) + half * LANES, LANES), LANES)

    blocks = [(own_ref, h, held, lanes_at(0, h)) for h in range(2)]
    for k in range(1, 4):
        for h in range(2):
            blocks.append((mine_ref, 2 * k - 2 + h, held, lanes_at(-way * k, h)))
            blocks.append((other_ref, 2 * k - 2 + h, slice(0, HALF), lanes_at(way * k, h)))
    blocks.append((mine_ref, 6, held, lanes_at(4, c)))
    blocks.append((other_ref, 6, slice(0, HALF), lanes_at(4, 1 - c)))
    totals_ref[...] = functools.reduce(
        jnp.add,
        [
            ref[i, HALF if ref is other_ref else SLOTS :, :].astype(f32)
            for ref, i, _, _ in blocks
        ],
    )
    total = square = 0.0
    for ref, i, rows, _ in blocks:
        v = ref[i, rows, :].astype(f32)
        total = total + v
        square = square + v * v
    center = jnp.sum(total, axis=1, keepdims=True) * (1.0 / D)
    spread = jnp.sum(square, axis=1, keepdims=True) * (1.0 / D) - center * center
    scale = lax.rsqrt(spread + NORM_EPS)
    offset = center * scale
    for ref, i, rows, lanes in blocks:
        v = ref[i, rows, :].astype(f32) * scale - offset
        rows_ref[:, lanes] = (v * affine_ref[0:1, lanes] + affine_ref[1:2, lanes]).astype(bf16)
    for i, (g, u) in enumerate(((gate_ref, up_ref), (gate_other_ref, up_other_ref))):
        gate = jnp.dot(rows_ref[...], g[...], preferred_element_type=f32)
        up = jnp.dot(rows_ref[...], u[...], preferred_element_type=f32)
        middle_ref[i] = (gate / (1.0 + jnp.exp(-gate)) * up).astype(bf16)
    project(middle_ref, down_ref, down_other_ref, send_ref, -way, 1 - c)


def project(middle_ref, down_ref, down_other_ref, out_ref, way, half):
    y = lax.axis_index("y")

    def down(away, begin, width):
        at = lax.rem(y + away + Y, Y) * 2 * LANES + begin
        lanes = pl.ds(pl.multiple_of(at, LANES), width)
        out = jnp.dot(middle_ref[0], down_ref[:, lanes], preferred_element_type=f32)
        return out + jnp.dot(middle_ref[1], down_other_ref[:, lanes], preferred_element_type=f32)

    for k in range(1, 4):
        out = down(way * k, 0, 2 * LANES)
        out_ref[2 * k - 2] = out[:, :LANES].astype(bf16)
        out_ref[2 * k - 1] = out[:, LANES:].astype(bf16)
    out_ref[6] = down(4, half * LANES, LANES).astype(bf16)
    out_ref[7] = down(0, half * LANES, LANES).astype(bf16)


def keep_kernel(middle_ref, down_ref, down_other_ref, keep_ref):
    c = lax.axis_index("c")
    project(middle_ref, down_ref, down_other_ref, keep_ref, 1 - 2 * c, c)


def combine_kernel(
    returned_ref, first_ref, totals_ref, slots_ref, logits_ref, gain_ref, shift_ref,
    second_ref, stats_ref,
):
    totals = totals_ref[...]
    totals = totals[0:4] + totals[4:8]
    sums, squares = [], []
    for h in range(2):
        rows = slice(h * LANES, (h + 1) * LANES)
        center = column(totals[h : h + 1]) * (1.0 / D)
        spread = column(totals[2 + h : 3 + h]) * (1.0 / D) - center * center
        hidden = (first_ref[rows, :] - center) * lax.rsqrt(spread + NORM_EPS)
        hidden = hidden * gain_ref[...] + shift_ref[...]
        slot = lax.broadcasted_iota(jnp.int32, (LANES, SLOTS), 1).astype(f32)
        logits = [column(logits_ref[r : r + 1, rows]) for r in range(TOP)]
        top = jnp.maximum(logits[0], logits[1])
        weights = [jnp.exp(v - top) for v in logits]
        norm = weights[0] + weights[1]
        moe = 0.0
        for r in range(TOP):
            at = column(slots_ref[r : r + 1, rows].astype(f32))
            place = (slot == at).astype(f32).astype(bf16)
            picked = jnp.dot(place, returned_ref[...], preferred_element_type=f32)
            moe = moe + weights[r] / norm * picked
        second = DEEP_ALPHA * hidden + moe
        second_ref[rows, :] = second
        sums.append(row_of(jnp.sum(second, axis=1, keepdims=True)))
        squares.append(row_of(jnp.sum(second * second, axis=1, keepdims=True)))
    stats = jnp.concatenate(sums + squares + [jnp.zeros((4, LANES), f32)], axis=0)
    for t in range(N_TP):
        stats_ref[t] = stats


def norm_kernel(stats_ref, second_ref, gain_ref, shift_ref, out_ref):
    totals = functools.reduce(jnp.add, [stats_ref[t] for t in range(N_TP)])
    for h in range(2):
        rows = slice(h * LANES, (h + 1) * LANES)
        center = column(totals[h : h + 1]) * (1.0 / D)
        spread = column(totals[2 + h : 3 + h]) * (1.0 / D) - center * center
        out = (second_ref[rows, :] - center) * lax.rsqrt(spread + NORM_EPS)
        out_ref[rows, :] = (out * gain_ref[...] + shift_ref[...]).astype(bf16)


def call(kernel, outs, flops, moved, limit=16 << 20, **more):
    return pl.pallas_call(
        kernel,
        out_shape=outs,
        cost_estimate=pl.CostEstimate(flops=flops, bytes_accessed=moved, transcendentals=0),
        compiler_params=pltpu.CompilerParams(vmem_limit_bytes=limit),
        **more,
    )


def shape(dims, dtype):
    return jax.ShapeDtypeStruct(dims, dtype)


def swap(v):
    return lax.ppermute(v, "c", [(0, 1), (1, 0)])


def onward(v, distance):
    pairs = []
    for y in range(Y):
        pairs.append((2 * y, 2 * ((y + distance) % Y)))
        pairs.append((2 * y + 1, 2 * ((y - distance) % Y) + 1))
    return lax.ppermute(v, TP, pairs)


def by_core(even, odd):
    return jnp.where(lax.axis_index("c") == 0, even, odd)


def to_all(value):
    return lax.all_to_all(value, TP, 0, 0, tiled=True)


def over_sp(value):
    return lax.all_to_all(value, SP, 0, 0, tiled=True)


def gather_columns(own):
    two = onward(own, 2)
    one = onward(own, 1)
    three = onward(two, 1)
    four = onward(by_core(two[0:1], two[1:2]), 2)
    mine = jnp.concatenate([one, two, three, four], axis=0)
    passed = by_core(mine[:, HALF:SLOTS], mine[:, :HALF])
    return own, mine, swap(jnp.concatenate([passed, mine[:, SLOTS:]], axis=1))


def scatter_sum(keep, passed):
    def full(begin, end):
        own, other = keep[begin:end], passed[begin:end]
        return by_core(
            jnp.concatenate([own, other], axis=1), jnp.concatenate([other, own], axis=1)
        )

    three = onward(full(4, 6), 1)
    four = onward(full(6, 7), 2)
    one = onward(full(0, 2), 1)
    four = four.astype(f32)
    none = jnp.zeros_like(four)
    four = by_core(jnp.concatenate([four, none]), jnp.concatenate([none, four]))
    two = onward((full(2, 4).astype(f32) + three.astype(f32) + four).astype(bf16), 2)
    side = one.astype(f32) + two.astype(f32)
    other = swap(by_core(side[1], side[0]).astype(bf16))
    return by_core(side[0], side[1]) + other.astype(f32) + full(7, 8)[0].astype(f32)


def local(
    residual, queries, keys, values, documents, sinks, head_gain, out_weight, norm_gain,
    norm_shift, routes, route_logits, gate_weight, up_weight, down_weight, final_gain,
    final_shift,
):
    docs = documents[None]
    hbm = pl.BlockSpec(memory_space=pltpu.HBM)
    halo = call(
        halo_kernel,
        shape((WINDOW + 8, 2 * LANES), bf16),
        1_000,
        140_000,
        limit=FULL - 160_000,
        in_specs=[hbm] * 3,
        scratch_shapes=[
            pltpu.VMEM((WINDOW, LANES), bf16),
            pltpu.VMEM((WINDOW, LANES), bf16),
            pltpu.VMEM((1, TOKENS), jnp.int32),
            pltpu.SemaphoreType.DMA((3,)),
        ],
    )(keys, values, docs)
    halo = lax.ppermute(halo, SP, [(i - 1, i) for i in range(1, N_SP)])
    gain, shift = norm_gain[None], norm_shift[None]
    prepared = call(
        prepare_kernel,
        shape((TOKENS + WINDOW + 24, LANES), bf16),
        3_000_000,
        600_000,
        limit=FULL - 240_000,
        in_specs=[hbm] * 9,
        scratch_shapes=[
            pltpu.VMEM((TOKENS, LANES), bf16),
            pltpu.VMEM((1024, LANES), bf16),
            pltpu.VMEM((1, LANES), f32),
            pltpu.VMEM((1, LANES), f32),
            pltpu.VMEM((TOKENS, LANES), bf16),
            pltpu.VMEM((TOKENS, LANES), bf16),
            pltpu.VMEM((HEAD_SIZE, TOKENS), bf16),
            pltpu.VMEM((1, TOKENS), jnp.int32),
            pltpu.VMEM((1, 1), f32),
            pltpu.SemaphoreType.DMA((9,)),
        ],
    )(residual, out_weight, gain, shift, keys, values, queries.T, docs, sinks[None])
    payload = call(
        attention_kernel, shape((Y, WINDOW + 16, LANES), bf16), 60_000_000, 1_000_000
    )(halo, prepared)
    gathered = lax.all_to_all(payload, "y", 0, 0, tiled=True)
    first, outgoing, stats, slots, affine = call(
        mix_kernel,
        (
            shape((TOKENS, LANES), f32),
            shape((SLOTS, LANES), bf16),
            shape((STAT_ROWS, LANES), bf16),
            shape((8, TOKENS), jnp.int32),
            shape((2, D), f32),
        ),
        140_000_000,
        1_500_000,
    )(gathered, swap(gathered), head_gain[None], out_weight, residual, routes.T)
    arrived = over_sp(outgoing.reshape(N_SP, CAP, LANES)).reshape(SLOTS, LANES)
    rows = SLOTS + STAT_ROWS
    block = call(block_kernel, shape((rows, LANES), bf16), 1_000, 400_000, limit=8 << 20)(
        arrived, stats
    )
    own = call(own_kernel, shape((2, rows, LANES), bf16), 1_000, 800_000, limit=8 << 20)(
        block, swap(block)
    )
    weights = (gate_weight[0], up_weight[0], down_weight[0])
    others = tuple(swap(w) for w in weights)
    blocks = shape((8, HALF, LANES), bf16)
    middle, send, totals = call(
        expert_kernel,
        (shape((2, HALF, FF_LOCAL), bf16), blocks, shape((STAT_ROWS, LANES), f32)),
        2 * HALF * D * FF_LOCAL * 5,
        14_000_000,
        limit=24 << 20,
        scratch_shapes=[pltpu.VMEM((HALF, D), bf16)],
    )(*gather_columns(own), affine, *weights, *others)
    passed = swap(send)
    keep = call(keep_kernel, blocks, 2 * HALF * D * FF_LOCAL, 5_000_000)(
        middle, weights[2], others[2]
    )
    summed = scatter_sum(keep, passed).astype(bf16)
    returned = over_sp(summed.reshape(N_SP, CAP, LANES)).reshape(SLOTS, LANES)
    second, last = call(
        combine_kernel,
        (shape((TOKENS, LANES), f32), shape((N_TP, 8, LANES), f32)),
        110_000_000,
        800_000,
    )(returned, first, totals, slots, route_logits.T, gain, shift)
    return call(norm_kernel, shape((TOKENS, LANES), bf16), 1_000_000, 400_000)(
        to_all(last), second, final_gain[None], final_shift[None]
    )


def solution(mesh):
    physical = Mesh(mesh.devices.reshape(8, 4, Y, 2), SP + TP)
    return jax.shard_map(
        local,
        mesh=physical,
        in_specs=(
            P(SP, TP),
            P(SP, TP),
            P(SP, None),
            P(SP, None),
            P(SP),
            P(TP),
            P(),
            P(None, TP),
            P(TP),
            P(TP),
            P(SP, None),
            P(SP, None),
            P(SP, None, TP),
            P(SP, None, TP),
            P(SP, TP, None),
            P(TP),
            P(TP),
        ),
        out_specs=P(SP, TP),
        check_vma=False,
    )
```
